32 devices in a mesh: grp: 2 (over y), tp: 4 (over z), dp: 4 (over x, core).
Axes of the slice: x: 2, y: 2, z: 4, core: 2. Of those that a mesh axis runs over, the one named last changes fastest.
Arguments:
- tokens: bfloat16 [64, 8, 4096], P(('grp', 'tp'), None, 'dp'), parts along dimension 0, may hold values from -6 to 6
- lengths: int32 [64], P('grp'), parts along dimension 0, may hold values from 1 to 8, 112 in all
- norm_gain: float32 [2, 4096], P(None, 'dp'), may hold values from 0.1 to 1.9
- w_recept: bfloat16 [2, 4096, 2048], P(None, 'dp', 'tp'), may hold values from -0.09375 to 0.09375
- w_key: bfloat16 [2, 4096, 2048], P(None, 'dp', 'tp'), may hold values from -0.09375 to 0.09375
- w_value: bfloat16 [2, 4096, 2048], P(None, 'dp', 'tp'), may hold values from -0.09375 to 0.09375
- w_decay: bfloat16 [2, 4096, 2048], P(None, 'dp', 'tp'), may hold values from -0.375 to 0.375
- w_rate: bfloat16 [2, 4096, 2048], P(None, 'dp', 'tp'), may hold values from -0.09375 to 0.09375
- w_gate: bfloat16 [2, 4096, 2048], P(None, 'dp', 'tp'), may hold values from -0.09375 to 0.09375
- w_out: bfloat16 [2, 2048, 4096], P(None, 'tp', 'dp'), may hold values from -0.125 to 0.125
- decay_base: float32 [2, 2048], P(None, 'tp'), may hold values from -4 to 3
- out_gain: float32 [2, 2048], P(None, 'tp'), may hold values from 0.1 to 1.9
- states: float32 [2, 64, 64, 2048], P(None, ('grp', 'dp'), None, 'tp'), parts along dimension 1, may hold values from -6 to 6
Outputs:
- stream_out: float32 [64, 8, 4096], P(('grp', 'tp'), None, 'dp'), parts along dimension 0
- new_states: float32 [2, 64, 64, 2048], P(None, ('grp', 'dp'), None, 'tp'), parts along dimension 1
The draws below stay inside these ranges and needn't reach their ends.
There are 2 independent parts, one for each index of `grp`. The reference program is written for one: setup_inputs(seed, part) draws one part's arguments, and reference() takes and returns one part's arrays. A program takes and returns all parts, laid end to end along the dimension named above; an argument that names none is the same for every part. Nothing has to cross between parts.
Inputs may be any that keep to these rules, and one draw needn't show every extreme that they name: lengths[b] first tokens of sequence b are live; together they count 7 * 16 and the largest is 8.
All inputs are finite; a program needn't handle non-finite values.
Results may differ from the reference program's by a relative error of at most 0.0061.
Values may be sent and summed in bfloat16 or wider, within the bound.
A program may use at most 128 MiB of HBM per device.

```python
import math
import jax
import jax.numpy as jnp
import numpy as np
from jax import lax

D = 4096
HEAD = 64
WIDTH = 2048
STEPS = 8
BLOCKS = 2
SEQS = 32


def draw_tokens(key, part):
    row_key, column_key, value_key = jax.random.split(key, 3)
    rising = jnp.exp(jnp.linspace(math.log(0.5), math.log(2.0), D))
    rough = jax.random.uniform(column_key, (D,), jnp.float32, 0.6, 1.5)
    row_scale = jnp.exp(jax.random.uniform(row_key, (SEQS, STEPS, 1), jnp.float32, math.log(0.1), math.log(1.0)))
    values = jax.random.normal(value_key, (SEQS, STEPS, D), jnp.float32)
    drawn = jnp.clip(values * row_scale * rising * rough, -6.0, 6.0)
    return drawn.astype(jnp.bfloat16)


def steps_of(key, shape, shards, least, high):
    def one(dim, parts):
        heights = jax.random.uniform(jax.random.fold_in(jax.random.fold_in(key, 6), dim), (parts,), jnp.float32, least / len(shards), high / len(shards))
        return jnp.repeat(jnp.exp(heights), shape[dim] // parts).reshape((-1,) + (1,) * (len(shape) - dim - 1))

    level = one(*shards[0])
    for cut in shards[1:]:
        level = level * one(*cut)
    return level


def length_profile(count, total, bound, skew):
    weights = [(1 << 20) // math.isqrt(grade ** skew) + 1 for grade in range(2, count + 1)]
    surplus, given = total - bound - (count - 1), [1] * (count - 1)
    while surplus > 0:
        movable = [i for i in range(count - 1) if given[i] < bound]
        whole, budget = sum([weights[i] for i in movable]), surplus
        for i in movable:
            extra = min(bound - given[i], max(1, budget * weights[i] // whole), surplus)
            given[i] = given[i] + extra
            surplus = surplus - extra
    return np.array([bound] + given)


def ragged_sizes(stream_key, number_of, total, most, skew):
    if number_of == 2:
        one = jax.random.randint(stream_key, (), max(1, total - most), min(most, total - 1) + 1)
        return jnp.stack([one, total - one])
    tallies = jnp.asarray(length_profile(number_of, total, most, skew), jnp.int32)
    twos = (number_of - 1) // 2
    donor, taker = tallies[1:1 + 2 * twos:2], tallies[2:2 + 2 * twos:2]
    margin = jnp.minimum(donor - 1, most - taker)
    moved = jax.random.randint(jax.random.fold_in(stream_key, 1), (twos,), 0, 1 << 20) % (margin + 1)
    tallies = tallies.at[1:1 + 2 * twos:2].set(donor - moved).at[2:2 + 2 * twos:2].set(taker + moved)
    return tallies[jax.random.permutation(jax.random.fold_in(stream_key, 2), number_of)]


def bell_draw(own_key, shape, deviation, reach, pieces=(), kind=jnp.bfloat16):
    gain = steps_of(own_key, shape, pieces, -0.22, 0.18) if pieces else 1.0
    array = jax.random.normal(own_key, shape, jnp.float32) * deviation * gain
    return jnp.minimum(jnp.maximum(array, -reach), reach).astype(kind)


def setup_inputs(seed: int = 0, part: int = 0) -> dict:
    arg_keys = jax.random.split(jax.random.key(seed), 14)
    part_splits = jax.random.split(jax.random.fold_in(arg_keys[13], part), 14)
    tokens = draw_tokens(jax.random.fold_in(jax.random.fold_in(arg_keys[13], part), 71), part)
    lengths = ragged_sizes(part_splits[1], SEQS, 7 * SEQS // 2, STEPS, 2).astype(jnp.int32)
    norm_gain = jnp.clip(1.0 + 0.18 * jax.random.normal(arg_keys[2], (BLOCKS, D), jnp.float32), 0.1, 1.9)
    w_recept = bell_draw(arg_keys[3], (BLOCKS, D, WIDTH), D ** -0.5, 0.09375, ((1, 4), (2, 4)))
    w_key = bell_draw(arg_keys[4], (BLOCKS, D, WIDTH), D ** -0.5, 0.09375, ((1, 4), (2, 4)))
    w_value = bell_draw(arg_keys[5], (BLOCKS, D, WIDTH), D ** -0.5, 0.09375, ((1, 4), (2, 4)))
    w_decay = bell_draw(arg_keys[6], (BLOCKS, D, WIDTH), (D // 16) ** -0.5, 0.375, ((1, 4), (2, 4)))
    w_rate = bell_draw(arg_keys[7], (BLOCKS, D, WIDTH), D ** -0.5, 0.09375, ((1, 4), (2, 4)))
    w_gate = bell_draw(arg_keys[8], (BLOCKS, D, WIDTH), D ** -0.5, 0.09375, ((1, 4), (2, 4)))
    w_out = bell_draw(arg_keys[9], (BLOCKS, WIDTH, D), WIDTH ** -0.5, 0.125, ((1, 4), (2, 4)))
    decay_base = jnp.clip(-4.0 + 7.0 * jax.random.uniform(arg_keys[10], (BLOCKS, WIDTH), jnp.float32) ** steps_of(arg_keys[10], (BLOCKS, WIDTH), ((1, 4),), -0.2, 0.2), -4.0, 3.0)
    out_gain = jnp.clip(1.0 + 0.18 * jax.random.normal(arg_keys[11], (BLOCKS, WIDTH), jnp.float32), 0.1, 1.9)
    states = bell_draw(part_splits[12], (BLOCKS, SEQS, HEAD, WIDTH), 1.0, 6.0, ((1, 4), (3, 4)), jnp.float32)
    return {"tokens": tokens, "lengths": lengths, "norm_gain": norm_gain, "w_recept": w_recept, "w_key": w_key, "w_value": w_value, "w_decay": w_decay, "w_rate": w_rate, "w_gate": w_gate, "w_out": w_out, "decay_base": decay_base, "out_gain": out_gain, "states": states}


group_eps = 0.00064
norm_eps = 1e-06
key_eps = 1e-06
decay_scale = 0.606531
highest = lax.Precision.HIGHEST

def mix_heads(state_in, recept, keys_in, values, decay_pre, rate_pre, gate_pre, base_shift, out_scale, live_mask, head_size):
    row_count, step_count, width_all = recept.shape
    head_count = width_all // head_size
    shape_heads = (row_count, step_count, head_count, head_size)
    decay_rate = jnp.exp(-decay_scale * jax.nn.sigmoid(decay_pre + base_shift)).reshape(shape_heads)
    learn_rate = jax.nn.sigmoid(rate_pre).reshape(shape_heads)
    key_heads = keys_in.reshape(shape_heads)
    unit_keys = key_heads * lax.rsqrt(lax.optimization_barrier(jnp.sum(key_heads * key_heads, axis=3, keepdims=True)) + key_eps)
    removal = unit_keys * learn_rate
    recept_heads = recept.reshape(shape_heads)
    value_heads = values.reshape(shape_heads)
    memory = state_in.reshape(row_count, head_size, head_count, head_size)
    outputs = []
    for position in range(step_count):
        seen_part = jnp.einsum('bihj,bhj->bhi', memory, unit_keys[:, position], precision=highest)
        updated = memory * decay_rate[:, position][:, None, :, :] - jnp.swapaxes(seen_part, 1, 2)[:, :, :, None] * removal[:, position][:, None, :, :] + jnp.swapaxes(value_heads[:, position], 1, 2)[:, :, :, None] * key_heads[:, position][:, None, :, :]
        memory = jnp.where(live_mask[:, position][:, None, None, None], updated, memory)
        outputs.append(jnp.einsum('bihj,bhj->bhi', memory, recept_heads[:, position], precision=highest))
    readout = jnp.stack(outputs, axis=1)
    centered = readout - lax.optimization_barrier(jnp.mean(readout, axis=3, keepdims=True))
    normed = centered * lax.rsqrt(lax.optimization_barrier(jnp.mean(centered * centered, axis=3, keepdims=True)) + group_eps)
    gated = normed.reshape(row_count, step_count, width_all) * out_scale * jax.nn.sigmoid(gate_pre)
    gated = jnp.where(live_mask[:, :, None], gated, 0.0)
    return (gated.astype(jnp.bfloat16), memory.reshape(row_count, head_size, width_all))

def reference(tokens, lengths, norm_gain, w_recept, w_key, w_value, w_decay, w_rate, w_gate, w_out, decay_base, out_gain, states):
    live_mask = jnp.arange(STEPS, dtype=jnp.int32)[None, :] < lengths[:, None]
    current = tokens.astype(jnp.float32)
    finals = []
    for block_index in range(BLOCKS):
        inv_rms = lax.rsqrt(lax.optimization_barrier(jnp.sum(current * current, axis=2)) / D + norm_eps)
        scaled = (current * norm_gain[block_index]).astype(jnp.bfloat16).reshape(SEQS * STEPS, D)
        projected = [jnp.dot(scaled, weight[block_index], preferred_element_type=jnp.float32).reshape(SEQS, STEPS, WIDTH) * inv_rms[:, :, None] for weight in (w_recept, w_key, w_value, w_decay, w_rate, w_gate)]
        gated, final_state = mix_heads(states[block_index], projected[0], projected[1], projected[2], projected[3], projected[4], projected[5], decay_base[block_index], out_gain[block_index], live_mask, HEAD)
        finals.append(final_state)
        output = jnp.dot(gated.reshape(SEQS * STEPS, WIDTH), w_out[block_index], preferred_element_type=jnp.float32).reshape(SEQS, STEPS, D)
        current = current + output
    return (current, jnp.stack(finals, axis=0))
```

```python
import functools

import jax
import jax.numpy as jnp
from jax import lax
from jax.experimental import pallas as pl
from jax.experimental.pallas import tpu as pltpu
from jax.sharding import PartitionSpec as P

HEAD = 64
BLOCKS = 2
LANES = 128
CORES = 2

group_eps = 0.00064
norm_eps = 1e-06
key_eps = 1e-06
decay_scale = 0.606531
MESH = pl.DeviceIdType.MESH
F32 = jnp.float32
BF16 = jnp.bfloat16


def remote(src, dst, send, recv, axis, peer):
    return pltpu.make_async_remote_copy(
        src_ref=src,
        dst_ref=dst,
        send_sem=send,
        recv_sem=recv,
        device_id={axis: peer},
        device_id_type=MESH,
    )


def greet(peers):
    barrier = pltpu.get_barrier_semaphore()
    for axis, peer in peers:
        pl.semaphore_signal(barrier, inc=1, device_id={axis: peer}, device_id_type=MESH)
    pl.semaphore_wait(barrier, len(peers))


def grid_of(shape, dim):
    return lax.broadcasted_iota(jnp.int32, shape, dim)


def dot(a, b, dims=(((1,), (0,)), ((), ()))):
    return lax.dot_general(a.astype(BF16), b.astype(BF16), dims, preferred_element_type=F32)


def exact(a, b, dims=(((1,), (0,)), ((), ()))):
    return lax.dot_general(
        a, b, dims, preferred_element_type=F32, precision=lax.Precision.HIGHEST
    )


def split_dot(a, b):
    hi = a.astype(BF16)
    lo = (a - hi.astype(F32)).astype(BF16)
    return jnp.dot(hi, b, preferred_element_type=F32) + jnp.dot(lo, b, preferred_element_type=F32)


NT = (((1,), (1,)), ((), ()))
TN = (((0,), (0,)), ((), ()))


def mix(
    features, steps, block, proj, total, live, base, gain, state, final, span,
    vals_s, seen_s, read_s, ask_s, on_s,
):
    rows = total.shape[0]
    held = rows // steps
    heads = span // HEAD
    tall = steps * heads
    inv = lax.rsqrt(jnp.sum(total, axis=1, keepdims=True) / features + norm_eps)
    recept, keys, values, decay_pre, rate_pre, gate_pre = (proj(i) * inv for i in range(6))
    seg = (grid_of((span, span), 0) // HEAD == grid_of((span, span), 1) // HEAD).astype(F32).astype(BF16)
    unit = keys * lax.rsqrt(split_dot(keys * keys, seg) + key_eps)
    removal = unit * jax.nn.sigmoid(rate_pre) * live
    logd = -decay_scale * jax.nn.sigmoid(decay_pre + base) * live
    step_of = grid_of((rows, 1), 0) % steps
    upto = logd
    shift = 1
    while shift < steps:
        upto = upto + jnp.where(step_of >= shift, pltpu.roll(upto, shift, 0), 0.0)
        shift *= 2
    grow = jnp.exp(upto)
    back = jnp.exp(-upto)
    u_in = unit * jnp.exp(upto - logd)
    q_in = recept * grow
    r_out = removal * back
    k_out = keys * live * back
    scale_out = gain * jax.nn.sigmoid(gate_pre) * live

    lane = grid_of((rows, LANES), 1)
    for j in range(span // LANES):
        pair = values[:, j * LANES : (j + 1) * LANES]
        vals_s[pl.ds(2 * j, rows, stride=heads), :] = pair
        vals_s[pl.ds(2 * j + 1, rows, stride=heads), :] = pltpu.roll(pair, HEAD, 1)

    if heads % 8 == 0:
        one = jnp.where(grid_of((heads, span), 0) == grid_of((heads, span), 1) // HEAD, 1.0, 0.0)

        def spread(a):
            return jnp.concatenate(
                [jnp.broadcast_to(a[s : s + 1], (heads, span)) * one for s in range(steps)], axis=0
            )
    else:
        pick = jnp.where(grid_of((tall, steps), 0) // heads == grid_of((tall, steps), 1), 1.0, 0.0)
        mask = jnp.where(grid_of((tall, span), 0) % heads == grid_of((tall, span), 1) // HEAD, 1.0, 0.0)

        def spread(a):
            return dot(pick, a) * mask

    pad = jnp.zeros((LANES - HEAD - 2 * steps, span), F32)
    ends = []
    for b in range(held):
        cut = slice(b * steps, (b + 1) * steps)
        ask_s[b, 0:tall, :] = spread(u_in[cut]).astype(BF16)
        ask_s[b, tall : 2 * tall, :] = spread(q_in[cut]).astype(BF16)
        ends.append(grow[(b + 1) * steps - 1 : (b + 1) * steps])
    for b in range(held):
        cut = slice(b * steps, (b + 1) * steps)
        against = jnp.concatenate([state[block, b], r_out[cut], k_out[cut], pad], axis=0)
        on_s[b] = dot(ask_s[b], against, NT)

    for b in range(held):
        first = b * tall
        vals = [vals_s[first + s * heads : first + (s + 1) * heads, :] for s in range(steps)]
        seen = []
        for s in range(steps):
            on = on_s[b, s * heads : (s + 1) * heads, :]
            acc = on
            for p in range(s):
                r = on[:, HEAD + p : HEAD + p + 1]
                k = on[:, HEAD + steps + p : HEAD + steps + p + 1]
                acc = acc + (k * vals[p] - r * seen[p])
            seen.append(acc)
            seen_s[first + s * heads : first + (s + 1) * heads, :] = acc
            on = on_s[b, tall + s * heads : tall + (s + 1) * heads, :]
            acc = on
            for p in range(s + 1):
                r = on[:, HEAD + p : HEAD + p + 1]
                k = on[:, HEAD + steps + p : HEAD + steps + p + 1]
                acc = acc + (k * vals[p] - r * seen[p])
            read_s[first + s * heads : first + (s + 1) * heads, :] = acc

    low = grid_of((held * tall, LANES), 1) < HEAD
    read = jnp.where(low, read_s[...], 0.0)
    mean = jnp.sum(read, axis=1, keepdims=True) / HEAD
    centered = jnp.where(low, read - mean, 0.0)
    var = jnp.sum(centered * centered, axis=1, keepdims=True) / HEAD
    read_s[...] = centered * lax.rsqrt(var + group_eps)
    flat = []
    for j in range(span // LANES):
        even = read_s[pl.ds(2 * j, rows, stride=heads), :]
        odd = read_s[pl.ds(2 * j + 1, rows, stride=heads), :]
        flat.append(jnp.where(lane < HEAD, even, pltpu.roll(odd, HEAD, 1)))
    gated = (jnp.concatenate(flat, axis=1) * scale_out).astype(BF16)

    def update():
        for b in range(held):
            cut = slice(b * steps, (b + 1) * steps)
            band = slice(b * tall, (b + 1) * tall)
            left = jnp.concatenate([vals_s[band, :], -seen_s[band, :]], axis=0)
            right = jnp.concatenate(
                [spread(k_out[cut] * ends[b]), spread(r_out[cut] * ends[b])], axis=0
            )
            final[block, b] = state[block, b] * ends[b] + dot(left, right, TN)[0:HEAD]

    return gated, update


def whole_kernel(
    ntp, ndp, steps, features, width,
    tokens, lengths, norm_gain, w0, w1, w2, w3, w4, w5, w_out, base_in, gain_in, states,
    out_ref, final_ref,
    xtok, lens, gains, bases, ogains, wbuf, wobuf, state,
    xg, sqg, part, send_a, recv_a, send_b, recv_b, sq_a, sq_ra, sq_b, sq_rb, totals,
    gg, osend, orecv, current,
    vals_s, seen_s, read_s, ask_s, on_s,
    load_sem, wsem, xs_sem, xr_sem, ss_sem, sr_sem, as_sem, ar_sem, bs_sem, br_sem,
    qas_sem, qar_sem, qbs_sem, qbr_sem, gs_sem, gr_sem, os_sem, or_sem,
):
    weights = (w0, w1, w2, w3, w4, w5)
    _, chunks, depth, _ = wbuf.shape
    halves = chunks // 6
    span = wobuf.shape[1]
    here = xg.shape[2]
    rows = totals.shape[0]
    held = rows // steps
    nx = ndp // CORES
    tp = lax.axis_index("tp")
    dp = lax.axis_index("dp")
    core = lax.rem(dp, CORES)
    xpos = dp // CORES
    partner = dp + 1 - 2 * core

    loads = [
        pltpu.make_async_copy(src, dst, load_sem.at[i])
        for i, (src, dst) in enumerate(
            (
                (tokens, xtok), (norm_gain, gains), (lengths, lens), (base_in, bases),
                (gain_in, ogains), (states, state), (w_out, wobuf),
            )
        )
    ]
    for cp in loads[:5]:
        cp.start()

    def load(block, c):
        return pltpu.make_async_copy(
            weights[c // halves].at[block, :, pl.ds((c % halves) * width, width)],
            wbuf.at[block, c],
            wsem.at[block, c],
        )

    for c in range(chunks):
        load(0, c).start()
    loads[5].start()
    loads[6].start()
    for block in range(1, BLOCKS):
        for c in range(chunks):
            load(block, c).start()
    greet(
        [("tp", lax.rem(tp + k, ntp)) for k in range(1, ntp)]
        + [("dp", lax.rem(dp + k, ndp)) for k in range(1, ndp)]
    )
    for cp in loads[:5]:
        cp.wait()
    current[...] = xtok[...].reshape(here, depth).astype(F32)
    seq_of = grid_of((rows, 1), 0) // steps
    count = jnp.zeros((rows, 1), jnp.int32)
    for b in range(held):
        count = jnp.where(seq_of == b, lens[dp * held + b], count)
    live = jnp.where(grid_of((rows, 1), 0) % steps < count, 1.0, 0.0)

    for block in range(BLOCKS):
        x = current[...]
        xg[block, tp] = (x * gains[block : block + 1, :]).astype(BF16)
        sq = x * x
        acc = sq[:, 0:LANES]
        for k in range(1, depth // LANES):
            acc = acc + sq[:, k * LANES : (k + 1) * LANES]
        sqg[block, tp] = acc

        gathers = []
        for k in range(1, ntp):
            peer = lax.rem(tp + k, ntp)
            cp = remote(
                xg.at[block, tp], xg.at[block, tp], xs_sem.at[block, k], xr_sem.at[block, k], "tp", peer
            )
            cq = remote(
                sqg.at[block, tp], sqg.at[block, tp], ss_sem.at[block, k], sr_sem.at[block, k], "tp", peer
            )
            cp.start()
            cq.start()
            gathers += [cp, cq]
        for k in range(1, ntp):
            src = lax.rem(tp + ntp - k, ntp)
            remote(
                xg.at[block, src], xg.at[block, src], xs_sem.at[block, k], xr_sem.at[block, k], "tp", src
            ).wait_recv()
            remote(
                sqg.at[block, src], sqg.at[block, src], ss_sem.at[block, k], sr_sem.at[block, k], "tp", src
            ).wait_recv()

        sq_all = sqg[block].reshape(ndp, rows, LANES)
        part_sq = [sq_all[d] for d in range(ndp)]

        def pick(parts, x_at, which):
            return jnp.where(which == 0, parts[CORES * x_at], parts[CORES * x_at + 1])

        for xd in range(nx):
            sq_a[block, xd] = pick(part_sq, xd, 1 - core)
            sq_b[block, xd] = pick(part_sq, xd, core)
        copy_qa = remote(
            sq_a.at[block], sq_ra.at[block], qas_sem.at[block], qar_sem.at[block], "dp", partner
        )
        copy_qa.start()

        def copy_a(c):
            return remote(
                send_a.at[block, c], recv_a.at[block, c], as_sem.at[block, c], ar_sem.at[block, c],
                "dp", partner,
            )

        def copy_b(c, k):
            xd = lax.rem(xpos + k, nx)
            return remote(
                send_b.at[block, c, k], recv_b.at[block, c, k],
                bs_sem.at[block, c, k], br_sem.at[block, c, k],
                "dp", CORES * xd + core,
            )

        def stage_b(c):
            copy_a(c).wait_recv()
            for k in range(1, nx):
                xd = lax.rem(xpos + k, nx)
                send_b[block, c, k] = (
                    part[c, CORES * xd + core] + recv_a[block, c, xd].astype(F32)
                ).astype(BF16)
                copy_b(c, k).start()

        def first(c, carry):
            pltpu.make_async_copy(wbuf.at[block, c], wbuf.at[block, c], wsem.at[block, c]).wait()
            res = jnp.dot(
                xg[block].reshape(ndp * rows, depth), wbuf[block, c], preferred_element_type=F32
            )
            part[c] = res.reshape(ndp, rows, width)
            for xd in range(nx):
                send_a[block, c, xd] = part[c, CORES * xd + 1 - core].astype(BF16)
            copy_a(c).start()

            @pl.when(c > 0)
            def _():
                stage_b(c - 1)

            return carry

        lax.fori_loop(0, chunks, first, 0)
        copy_qa.wait_recv()
        for xd in range(nx):
            sq_b[block, xd] = sq_b[block, xd] + sq_ra[block, xd]
        qb = []
        for k in range(1, nx):
            xd = lax.rem(xpos + k, nx)
            cp = remote(
                sq_b.at[block, xd], sq_rb.at[block, k], qbs_sem.at[block, k], qbr_sem.at[block, k],
                "dp", CORES * xd + core,
            )
            cp.start()
            qb.append(cp)
        stage_b(chunks - 1)

        def last(c, carry):
            own = part[c, CORES * xpos + core] + recv_a[block, c, xpos].astype(F32)
            for k in range(1, nx):
                copy_b(c, k).wait_recv()
                own = own + recv_b[block, c, k].astype(F32)
            totals[:, pl.ds(pl.multiple_of(c * width, width), width)] = own
            copy_a(c).wait_send()
            for k in range(1, nx):
                copy_b(c, k).wait_send()
            return carry

        lax.fori_loop(0, chunks, last, 0)
        total = sq_b[block, xpos]
        for k in range(1, nx):
            qb[k - 1].wait_recv()
            total = total + sq_rb[block, k]

        if block == 0:
            loads[5].wait()
            loads[6].wait()
        gated, update = mix(
            features, steps, block, lambda i: totals[:, i * span : (i + 1) * span], total, live,
            bases[block : block + 1, :], ogains[block : block + 1, :], state, final_ref, span,
            vals_s, seen_s, read_s, ask_s, on_s,
        )
        gg[block, dp] = gated
        shares = []
        for k in range(1, ndp):
            cp = remote(
                gg.at[block, dp], gg.at[block, dp], gs_sem.at[block, k], gr_sem.at[block, k],
                "dp", lax.rem(dp + k, ndp),
            )
            cp.start()
            shares.append(cp)
        update()
        for k in range(1, ndp):
            src = lax.rem(dp + ndp - k, ndp)
            remote(
                gg.at[block, src], gg.at[block, src], gs_sem.at[block, k], gr_sem.at[block, k], "dp", src
            ).wait_recv()
        every = gg.at[block].reshape(ntp, here, span)

        def partial_of(peer):
            return jnp.dot(every[peer], wobuf[block], preferred_element_type=F32)

        def copy_o(k):
            return remote(
                osend.at[block, k], orecv.at[block, k], os_sem.at[block, k], or_sem.at[block, k],
                "tp", lax.rem(tp + k, ntp),
            )

        def give(k, carry):
            osend[block, k] = partial_of(lax.rem(tp + k, ntp)).astype(BF16)
            copy_o(k).start()
            return carry

        lax.fori_loop(1, ntp, give, 0)
        current[...] += partial_of(tp)

        def take(k, carry):
            copy_o(k).wait_recv()
            current[...] += orecv[block, k].astype(F32)
            copy_o(k).wait_send()
            return carry

        lax.fori_loop(1, ntp, take, 0)
        copy_qa.wait_send()
        for cp in qb + gathers + shares:
            cp.wait_send()
    out_ref[...] = current[...].reshape(out_ref.shape)


def body(
    ntp, ndp,
    tokens, lengths, norm_gain,
    w_recept, w_key, w_value, w_decay, w_rate, w_gate,
    w_out, decay_base, out_gain, states,
):
    seqs, steps, depth = tokens.shape
    held = states.shape[1]
    rows = held * steps
    here = seqs * steps
    features = depth * ndp
    span = w_key.shape[2]
    width = min(256, span)
    chunks = 6 * span // width
    nx = ndp // CORES
    heads = span // HEAD
    tall = steps * heads
    dma = pltpu.SemaphoreType.DMA
    vmem = pl.BlockSpec(memory_space=pltpu.VMEM)
    hbm = pl.BlockSpec(memory_space=pl.ANY)
    B = BLOCKS

    def buf(*shape, dtype=F32):
        return pltpu.VMEM(shape, dtype)

    return pl.pallas_call(
        functools.partial(whole_kernel, ntp, ndp, steps, features, width),
        out_shape=(
            jax.ShapeDtypeStruct((seqs, steps, depth), F32),
            jax.ShapeDtypeStruct(states.shape, F32),
        ),
        in_specs=[hbm] * 13,
        out_specs=(vmem, vmem),
        scratch_shapes=[
            buf(seqs, steps, depth, dtype=BF16),
            pltpu.SMEM(lengths.shape, jnp.int32),
            buf(B, depth), buf(B, span), buf(B, span),
            buf(B, chunks, depth, width, dtype=BF16),
            buf(B, span, depth, dtype=BF16),
            buf(*states.shape),
            buf(B, ntp, here, depth, dtype=BF16),
            buf(B, ntp, here, LANES),
            buf(chunks, ndp, rows, width),
            buf(B, chunks, nx, rows, width, dtype=BF16),
            buf(B, chunks, nx, rows, width, dtype=BF16),
            buf(B, chunks, nx, rows, width, dtype=BF16),
            buf(B, chunks, nx, rows, width, dtype=BF16),
            buf(B, nx, rows, LANES), buf(B, nx, rows, LANES),
            buf(B, nx, rows, LANES), buf(B, nx, rows, LANES),
            buf(rows, 6 * span),
            buf(B, ndp, rows, span, dtype=BF16),
            buf(B, ntp, here, depth, dtype=BF16),
            buf(B, ntp, here, depth, dtype=BF16),
            buf(here, depth),
            buf(held * tall, LANES), buf(held * tall, LANES), buf(held * tall, LANES),
            buf(held, 2 * tall, span, dtype=BF16), buf(held, 2 * tall, LANES),
            dma((7,)), dma((B, chunks)),
            dma((B, ntp)), dma((B, ntp)), dma((B, ntp)), dma((B, ntp)),
            dma((B, chunks)), dma((B, chunks)),
            dma((B, chunks, nx)), dma((B, chunks, nx)),
            dma((B,)), dma((B,)), dma((B, nx)), dma((B, nx)),
            dma((B, ndp)), dma((B, ndp)), dma((B, ntp)), dma((B, ntp)),
        ],
        compiler_params=pltpu.CompilerParams(
            collective_id=0, has_side_effects=True, vmem_limit_bytes=60 * 1024 * 1024
        ),
        name="whole",
    )(
        tokens, lengths, norm_gain,
        w_recept, w_key, w_value, w_decay, w_rate, w_gate,
        w_out, decay_base, out_gain, states,
    )


def solution(mesh):
    in_specs = (
        P(("grp", "tp"), None, "dp"),
        P("grp"),
        P(None, "dp"),
        P(None, "dp", "tp"),
        P(None, "dp", "tp"),
        P(None, "dp", "tp"),
        P(None, "dp", "tp"),
        P(None, "dp", "tp"),
        P(None, "dp", "tp"),
        P(None, "tp", "dp"),
        P(None, "tp"),
        P(None, "tp"),
        P(None, ("grp", "dp"), None, "tp"),
    )
    out_specs = (P(("grp", "tp"), None, "dp"), P(None, ("grp", "dp"), None, "tp"))
    run = functools.partial(body, mesh.shape["tp"], mesh.shape["dp"])
    return jax.shard_map(run, mesh=mesh, in_specs=in_specs, out_specs=out_specs, check_vma=False)
```

```python
import functools

import jax
import jax.numpy as jnp
from jax import lax
from jax.experimental import pallas as pl
from jax.experimental.pallas import tpu as pltpu
from jax.sharding import PartitionSpec as P

HEAD = 64
BLOCKS = 2
LANES = 128
CORES = 2

group_eps = 0.00064
norm_eps = 1e-06
key_eps = 1e-06
decay_scale = 0.606531
MESH = pl.DeviceIdType.MESH
F32 = jnp.float32
BF16 = jnp.bfloat16


def remote(src, dst, send, recv, axis, peer):
    return pltpu.make_async_remote_copy(
        src_ref=src,
        dst_ref=dst,
        send_sem=send,
        recv_sem=recv,
        device_id={axis: peer},
        device_id_type=MESH,
    )


def greet(peers):
    barrier = pltpu.get_barrier_semaphore()
    for axis, peer in peers:
        pl.semaphore_signal(barrier, inc=1, device_id={axis: peer}, device_id_type=MESH)
    pl.semaphore_wait(barrier, len(peers))


def grid_of(shape, dim):
    return lax.broadcasted_iota(jnp.int32, shape, dim)


def dot(a, b, dims=(((1,), (0,)), ((), ()))):
    return lax.dot_general(a.astype(BF16), b.astype(BF16), dims, preferred_element_type=F32)


def exact(a, b, dims=(((1,), (0,)), ((), ()))):
    return lax.dot_general(
        a, b, dims, preferred_element_type=F32, precision=lax.Precision.HIGHEST
    )


def split_dot(a, b):
    hi = a.astype(BF16)
    lo = (a - hi.astype(F32)).astype(BF16)
    return jnp.dot(hi, b, preferred_element_type=F32) + jnp.dot(lo, b, preferred_element_type=F32)


def split_right(a, b):
    hi = b.astype(BF16)
    lo = (b - hi.astype(F32)).astype(BF16)
    return jnp.dot(a, hi, preferred_element_type=F32) + jnp.dot(a, lo, preferred_element_type=F32)


def by_index(values, index):
    out = jnp.full(index.shape, values[0], jnp.int32)
    for i in range(1, len(values)):
        out = jnp.where(index == i, values[i], out)
    return out


def lane_sums(x):
    sq = x * x
    acc = sq[:, 0:LANES]
    for k in range(1, x.shape[1] // LANES):
        acc = acc + sq[:, k * LANES : (k + 1) * LANES]
    return acc


NT = (((1,), (1,)), ((), ()))
TN = (((0,), (0,)), ((), ()))


def mix(
    steps, block, projected, live, base, gain, state, final, span,
    vals_s, seen_s, read_s, ask_s, on_s,
):
    recept, keys, values, decay_pre, rate_pre, gate_pre = projected
    rows = recept.shape[0]
    held = rows // steps
    heads = span // HEAD
    tall = steps * heads
    seg = (grid_of((span, span), 0) // HEAD == grid_of((span, span), 1) // HEAD).astype(F32).astype(BF16)
    unit = keys * lax.rsqrt(split_dot(keys * keys, seg) + key_eps)
    removal = unit * jax.nn.sigmoid(rate_pre) * live
    logd = -decay_scale * jax.nn.sigmoid(decay_pre + base) * live
    step_of = grid_of((rows, 1), 0) % steps
    upto = logd
    shift = 1
    while shift < steps:
        upto = upto + jnp.where(step_of >= shift, pltpu.roll(upto, shift, 0), 0.0)
        shift *= 2
    grow = jnp.exp(upto)
    back = jnp.exp(-upto)
    u_in = unit * jnp.exp(upto - logd)
    q_in = recept * grow
    r_out = removal * back
    k_out = keys * live * back
    scale_out = gain * jax.nn.sigmoid(gate_pre) * live

    lane = grid_of((rows, LANES), 1)
    for j in range(span // LANES):
        pair = values[:, j * LANES : (j + 1) * LANES]
        vals_s[pl.ds(2 * j, rows, stride=heads), :] = pair
        vals_s[pl.ds(2 * j + 1, rows, stride=heads), :] = pltpu.roll(pair, HEAD, 1)

    if heads % 8 == 0:
        one = jnp.where(grid_of((heads, span), 0) == grid_of((heads, span), 1) // HEAD, 1.0, 0.0)

        def spread(a):
            return jnp.concatenate(
                [jnp.broadcast_to(a[s : s + 1], (heads, span)) * one for s in range(steps)], axis=0
            )
    else:
        pick = jnp.where(grid_of((tall, steps), 0) // heads == grid_of((tall, steps), 1), 1.0, 0.0)
        mask = jnp.where(grid_of((tall, span), 0) % heads == grid_of((tall, span), 1) // HEAD, 1.0, 0.0)

        def spread(a):
            return dot(pick, a) * mask

    pad = jnp.zeros((LANES - HEAD - 2 * steps, span), F32)
    ends = []
    for b in range(held):
        cut = slice(b * steps, (b + 1) * steps)
        ask_s[b, 0:tall, :] = spread(u_in[cut]).astype(BF16)
        ask_s[b, tall : 2 * tall, :] = spread(q_in[cut]).astype(BF16)
        ends.append(grow[(b + 1) * steps - 1 : (b + 1) * steps])
    for b in range(held):
        cut = slice(b * steps, (b + 1) * steps)
        against = jnp.concatenate([state[block, b], r_out[cut], k_out[cut], pad], axis=0)
        on_s[b] = dot(ask_s[b], against, NT)

    for b in range(held):
        first = b * tall
        vals = [vals_s[first + s * heads : first + (s + 1) * heads, :] for s in range(steps)]
        seen = []
        for s in range(steps):
            on = on_s[b, s * heads : (s + 1) * heads, :]
            acc = on
            for p in range(s):
                r = on[:, HEAD + p : HEAD + p + 1]
                k = on[:, HEAD + steps + p : HEAD + steps + p + 1]
                acc = acc + (k * vals[p] - r * seen[p])
            seen.append(acc)
            seen_s[first + s * heads : first + (s + 1) * heads, :] = acc
            on = on_s[b, tall + s * heads : tall + (s + 1) * heads, :]
            acc = on
            for p in range(s + 1):
                r = on[:, HEAD + p : HEAD + p + 1]
                k = on[:, HEAD + steps + p : HEAD + steps + p + 1]
                acc = acc + (k * vals[p] - r * seen[p])
            read_s[first + s * heads : first + (s + 1) * heads, :] = acc

    low = grid_of((held * tall, LANES), 1) < HEAD
    read = jnp.where(low, read_s[...], 0.0)
    mean = jnp.sum(read, axis=1, keepdims=True) / HEAD
    centered = jnp.where(low, read - mean, 0.0)
    var = jnp.sum(centered * centered, axis=1, keepdims=True) / HEAD
    read_s[...] = centered * lax.rsqrt(var + group_eps)
    flat = []
    for j in range(span // LANES):
        even = read_s[pl.ds(2 * j, rows, stride=heads), :]
        odd = read_s[pl.ds(2 * j + 1, rows, stride=heads), :]
        flat.append(jnp.where(lane < HEAD, even, pltpu.roll(odd, HEAD, 1)))
    gated = (jnp.concatenate(flat, axis=1) * scale_out).astype(BF16)

    def update():
        for b in range(held):
            cut = slice(b * steps, (b + 1) * steps)
            band = slice(b * tall, (b + 1) * tall)
            left = jnp.concatenate([vals_s[band, :], -seen_s[band, :]], axis=0)
            right = jnp.concatenate(
                [spread(k_out[cut] * ends[b]), spread(r_out[cut] * ends[b])], axis=0
            )
            final[block, b] = state[block, b] * ends[b] + dot(left, right, TN)[0:HEAD]

    return gated, update


def whole_kernel(
    ntp, ndp, steps, features, width, cap, share,
    tokens, lengths, norm_gain, w0, w1, w2, w3, w4, w5, w_out, base_in, gain_in, states,
    out_ref, final_ref,
    xtok, lens, gains, bases, ogains, wbuf, wobuf, state,
    xg, xpk, sqpk, sqd, accpk, packer, unpacker, xall, part,
    send_a, recv_a, send_b, recv_b, totals,
    gg, osend, orecv, psend, precv,
    vals_s, seen_s, read_s, ask_s, on_s,
    load_sem, wsem, xs_sem, xr_sem, ss_sem, sr_sem, as_sem, ar_sem, bs_sem, br_sem,
    qs_sem, qr_sem, gs_sem, gr_sem, os_sem, or_sem,
):
    weights = (w0, w1, w2, w3, w4, w5)
    _, chunks, depth, _ = wbuf.shape
    halves = chunks // 6
    span = wobuf.shape[1]
    rows = totals.shape[0]
    held = state.shape[1]
    seqs = xtok.shape[0]
    natural = held * steps
    here = seqs * steps
    every = ntp * cap
    packed = ntp * share
    nx = ndp // CORES
    tp = lax.axis_index("tp")
    dp = lax.axis_index("dp")
    core = lax.rem(dp, CORES)
    xpos = dp // CORES
    partner = dp + 1 - 2 * core

    loads = [
        pltpu.make_async_copy(src, dst, load_sem.at[i])
        for i, (src, dst) in enumerate(
            (
                (tokens, xtok), (lengths, lens), (norm_gain, gains), (base_in, bases),
                (gain_in, ogains), (states, state), (w_out, wobuf),
            )
        )
    ]
    for cp in loads[:5]:
        cp.start()

    def load(block, c):
        return pltpu.make_async_copy(
            weights[c // halves].at[block, :, pl.ds((c % halves) * width, width)],
            wbuf.at[block, c],
            wsem.at[block, c],
        )

    for c in range(chunks):
        load(0, c).start()
    loads[5].start()
    loads[6].start()
    for block in range(1, BLOCKS):
        for c in range(chunks):
            load(block, c).start()
    greet(
        [("tp", lax.rem(tp + k, ntp)) for k in range(1, ntp)]
        + [("dp", lax.rem(dp + k, ndp)) for k in range(1, ndp)]
    )
    for cp in loads[:2]:
        cp.wait()

    def spot(first, number):
        index = grid_of((number * steps, 1), 0)
        at, starts, counts = jnp.int32(0), [], []
        for b in range(number):
            if b % seqs == 0:
                at = jnp.int32(b // seqs * cap)
            starts.append(at)
            counts.append(lens[first + b])
            at = at + counts[-1]
        step = index % steps
        place = by_index(starts, index // steps) + step
        alive = step < by_index(counts, index // steps)
        wide = (number * steps, number // seqs * cap)
        one = jnp.where((place == grid_of(wide, 1)) & alive, 1.0, 0.0)
        return one, jnp.where(alive, 1.0, 0.0)

    mine, mine_live = spot(tp * seqs, seqs)
    mine = mine.astype(BF16)
    flat_tokens = xtok[...].reshape(here, depth)
    xg[tp] = dot(mine, flat_tokens, TN).astype(BF16)
    sends = []

    def gather(buf, k, send, recv):
        cp = remote(buf.at[tp], buf.at[tp], send.at[k], recv.at[k], "tp", lax.rem(tp + k, ntp))
        cp.start()
        sends.append(cp)

    def gathered(buf, k, send, recv):
        src = lax.rem(tp + ntp - k, ntp)
        remote(buf.at[src], buf.at[src], send.at[k], recv.at[k], "tp", src).wait_recv()

    for k in range(1, ntp):
        gather(xg, k, xs_sem.at[0], xr_sem.at[0])

    own_spot, live = spot(dp * held, held)
    own_spot = own_spot.astype(BF16)
    starts, counts, at = [], [], jnp.int32(0)
    for g in range(ntp):
        starts.append(at)
        number = jnp.int32(0)
        for b in range(seqs):
            number = number + lens[g * seqs + b]
        counts.append(number)
        at = at + number

    def ranks(index):
        return jnp.where(
            index % cap < by_index(counts, index // cap),
            by_index(starts, index // cap) + index % cap,
            -1,
        )

    packer[...] = jnp.where(
        grid_of((packed, every), 0) == ranks(grid_of((1, every), 1)), 1.0, 0.0
    )
    unpacker[...] = jnp.where(
        ranks(grid_of((every, 1), 0)) == grid_of((every, packed), 1), 1.0, 0.0
    ).astype(BF16)
    accpk[...] = jnp.zeros_like(accpk)
    own_lanes = jnp.where(
        grid_of((rows, every), 1) == grid_of((rows, every), 0) + dp * rows, 1.0, 0.0
    )
    ones = jnp.ones((8, LANES), F32)
    for cp in loads[2:5]:
        cp.wait()
    for k in range(1, ntp):
        gathered(xg, k, xs_sem.at[0], xr_sem.at[0])
    part_rows = pl.ds(pl.multiple_of(tp * share, share), share)
    current = None

    for block in range(BLOCKS):
        if block == 0:
            x = xg[...].reshape(every, depth).astype(F32)
            xall[...] = (x * gains[0:1, :]).astype(BF16)
            sqd[block, dp] = exact(ones, lane_sums(x), NT)
        else:
            xpk[tp] = (current * gains[block : block + 1, :]).astype(BF16)
            accpk[part_rows, :] = lane_sums(current)
            sqpk[tp] = exact(ones, accpk[...], NT)
            for k in range(1, ntp):
                gather(xpk, k, xs_sem.at[1], xr_sem.at[1])
                gather(sqpk, k, ss_sem, sr_sem)
            for k in range(1, ntp):
                gathered(sqpk, k, ss_sem, sr_sem)
                gathered(xpk, k, xs_sem.at[1], xr_sem.at[1])
            xall[...] = dot(unpacker[...], xpk[...].reshape(packed, depth)).astype(BF16)
            sqd[block, dp] = exact(jnp.sum(sqpk[...], axis=0), packer[...])
        for k in range(1, ndp):
            cp = remote(
                sqd.at[block, dp], sqd.at[block, dp], qs_sem.at[block, k], qr_sem.at[block, k],
                "dp", lax.rem(dp + k, ndp),
            )
            cp.start()
            sends.append(cp)

        def copy_a(c):
            return remote(
                send_a.at[block, c], recv_a.at[block, c], as_sem.at[block, c], ar_sem.at[block, c],
                "dp", partner,
            )

        def copy_b(c, k):
            xd = lax.rem(xpos + k, nx)
            return remote(
                send_b.at[block, c, k], recv_b.at[block, c, k],
                bs_sem.at[block, c, k], br_sem.at[block, c, k],
                "dp", CORES * xd + core,
            )

        def stage_b(c):
            copy_a(c).wait_recv()
            for k in range(1, nx):
                xd = lax.rem(xpos + k, nx)
                send_b[block, c, k] = (
                    part[c, CORES * xd + core] + recv_a[block, c, xd].astype(F32)
                ).astype(BF16)
                copy_b(c, k).start()

        def first(c, carry):
            pltpu.make_async_copy(wbuf.at[block, c], wbuf.at[block, c], wsem.at[block, c]).wait()
            res = jnp.dot(xall[...], wbuf[block, c], preferred_element_type=F32)
            part[c] = res.reshape(ndp, rows, width)
            for xd in range(nx):
                send_a[block, c, xd] = part[c, CORES * xd + 1 - core].astype(BF16)
            copy_a(c).start()

            @pl.when(c > 0)
            def _():
                stage_b(c - 1)

            return carry

        lax.fori_loop(0, chunks, first, 0)
        stage_b(chunks - 1)
        for k in range(1, ndp):
            src = lax.rem(dp + ndp - k, ndp)
            remote(
                sqd.at[block, src], sqd.at[block, src], qs_sem.at[block, k], qr_sem.at[block, k],
                "dp", src,
            ).wait_recv()
        total = exact(own_lanes, jnp.sum(sqd[block], axis=0), NT)[:, 0:1]
        inv = lax.rsqrt(total / features + norm_eps)

        def last(c, carry):
            own = part[c, CORES * xpos + core] + recv_a[block, c, xpos].astype(F32)
            for k in range(1, nx):
                copy_b(c, k).wait_recv()
                own = own + recv_b[block, c, k].astype(F32)
            totals[:, pl.ds(pl.multiple_of(c * width, width), width)] = own * inv
            copy_a(c).wait_send()
            for k in range(1, nx):
                copy_b(c, k).wait_send()
            return carry

        lax.fori_loop(0, chunks, last, 0)
        if block == 0:
            loads[5].wait()
            loads[6].wait()
        gated, update = mix(
            steps, block,
            [split_right(own_spot, totals[:, i * span : (i + 1) * span]) for i in range(6)],
            live, bases[block : block + 1, :], ogains[block : block + 1, :], state, final_ref, span,
            vals_s, seen_s, read_s, ask_s, on_s,
        )
        gg[block, dp] = dot(own_spot, gated, TN).astype(BF16)
        for k in range(1, ndp):
            cp = remote(
                gg.at[block, dp], gg.at[block, dp], gs_sem.at[block, k], gr_sem.at[block, k],
                "dp", lax.rem(dp + k, ndp),
            )
            cp.start()
            sends.append(cp)
        update()
        if block + 1 < BLOCKS:
            current = dot(packer[part_rows, :], xg[...].reshape(every, depth))
        else:
            back = dot(
                unpacker[pl.ds(pl.multiple_of(tp * cap, cap), cap), :],
                xpk[...].reshape(packed, depth),
            )
            current = back / gains[block : block + 1, :]
        for k in range(1, ndp):
            src = lax.rem(dp + ndp - k, ndp)
            remote(
                gg.at[block, src], gg.at[block, src], gs_sem.at[block, k], gr_sem.at[block, k], "dp", src
            ).wait_recv()
        rest = gg[block].reshape(every, span)
        if block + 1 < BLOCKS:
            rest = dot(packer[...], rest).astype(BF16)
            sbuf, rbuf = psend, precv
        else:
            sbuf, rbuf = osend, orecv
        size = sbuf.shape[1]
        partial = jnp.dot(rest, wobuf[block], preferred_element_type=F32)
        for g in range(ntp):
            sbuf[g] = partial[g * size : (g + 1) * size].astype(BF16)
        back_sends = []
        for k in range(1, ntp):
            peer = lax.rem(tp + k, ntp)
            cp = remote(
                sbuf.at[peer], rbuf.at[k], os_sem.at[block, k], or_sem.at[block, k], "tp", peer
            )
            cp.start()
            sends.append(cp)
            back_sends.append(cp)
        for g in range(ntp):
            current = current + jnp.where(tp == g, partial[g * size : (g + 1) * size], 0.0)
        for k in range(1, ntp):
            back_sends[k - 1].wait_recv()
            current = current + rbuf[k].astype(F32)
    result = jnp.where(
        mine_live > 0, exact(mine.astype(F32), current), flat_tokens.astype(F32)
    )
    out_ref[...] = result.reshape(out_ref.shape)
    for cp in sends:
        cp.wait_send()


def body(
    ntp, ndp,
    tokens, lengths, norm_gain,
    w_recept, w_key, w_value, w_decay, w_rate, w_gate,
    w_out, decay_base, out_gain, states,
):
    seqs, steps, depth = tokens.shape
    held = states.shape[1]
    live_rows = 7 * lengths.shape[0] // 2
    cap = seqs * steps
    share = 16 * -(-live_rows // (16 * ntp))
    rows = ntp // ndp * cap
    features = depth * ndp
    span = w_key.shape[2]
    width = min(256, span)
    chunks = 6 * span // width
    nx = ndp // CORES
    heads = span // HEAD
    tall = steps * heads
    every = ntp * cap
    packed = ntp * share
    dma = pltpu.SemaphoreType.DMA
    vmem = pl.BlockSpec(memory_space=pltpu.VMEM)
    hbm = pl.BlockSpec(memory_space=pl.ANY)
    B = BLOCKS

    def buf(*shape, dtype=F32):
        return pltpu.VMEM(shape, dtype)

    return pl.pallas_call(
        functools.partial(whole_kernel, ntp, ndp, steps, features, width, cap, share),
        out_shape=(
            jax.ShapeDtypeStruct((seqs, steps, depth), F32),
            jax.ShapeDtypeStruct(states.shape, F32),
        ),
        in_specs=[hbm] * 13,
        out_specs=(vmem, vmem),
        scratch_shapes=[
            buf(seqs, steps, depth, dtype=BF16),
            pltpu.SMEM(lengths.shape, jnp.int32),
            buf(B, depth), buf(B, span), buf(B, span),
            buf(B, chunks, depth, width, dtype=BF16),
            buf(B, span, depth, dtype=BF16),
            buf(*states.shape),
            buf(ntp, cap, depth, dtype=BF16),
            buf(ntp, share, depth, dtype=BF16),
            buf(ntp, 8, packed),
            buf(B, ndp, 8, every),
            buf(packed, LANES),
            buf(packed, every), buf(every, packed, dtype=BF16),
            buf(every, depth, dtype=BF16),
            buf(chunks, ndp, rows, width),
            buf(B, chunks, nx, rows, width, dtype=BF16),
            buf(B, chunks, nx, rows, width, dtype=BF16),
            buf(B, chunks, nx, rows, width, dtype=BF16),
            buf(B, chunks, nx, rows, width, dtype=BF16),
            buf(rows, 6 * span),
            buf(B, ndp, rows, span, dtype=BF16),
            buf(ntp, cap, depth, dtype=BF16),
            buf(ntp, cap, depth, dtype=BF16),
            buf(ntp, share, depth, dtype=BF16),
            buf(ntp, share, depth, dtype=BF16),
            buf(held * tall, LANES), buf(held * tall, LANES), buf(held * tall, LANES),
            buf(held, 2 * tall, span, dtype=BF16), buf(held, 2 * tall, LANES),
            dma((7,)), dma((B, chunks)),
            dma((2, ntp)), dma((2, ntp)), dma((ntp,)), dma((ntp,)),
            dma((B, chunks)), dma((B, chunks)),
            dma((B, chunks, nx)), dma((B, chunks, nx)),
            dma((B, ndp)), dma((B, ndp)),
            dma((B, ndp)), dma((B, ndp)), dma((B, ntp)), dma((B, ntp)),
        ],
        compiler_params=pltpu.CompilerParams(
            collective_id=0, has_side_effects=True, vmem_limit_bytes=60 * 1024 * 1024
        ),
        name="whole",
    )(
        tokens, lengths, norm_gain,
        w_recept, w_key, w_value, w_decay, w_rate, w_gate,
        w_out, decay_base, out_gain, states,
    )


def solution(mesh):
    in_specs = (
        P(("grp", "tp"), None, "dp"),
        P("grp"),
        P(None, "dp"),
        P(None, "dp", "tp"),
        P(None, "dp", "tp"),
        P(None, "dp", "tp"),
        P(None, "dp", "tp"),
        P(None, "dp", "tp"),
        P(None, "dp", "tp"),
        P(None, "tp", "dp"),
        P(None, "tp"),
        P(None, "tp"),
        P(None, ("grp", "dp"), None, "tp"),
    )
    out_specs = (P(("grp", "tp"), None, "dp"), P(None, ("grp", "dp"), None, "tp"))
    run = functools.partial(body, mesh.shape["tp"], mesh.shape["dp"])
    return jax.shard_map(run, mesh=mesh, in_specs=in_specs, out_specs=out_specs, check_vma=False)
```

```python
import functools

import jax
import jax.numpy as jnp
from jax import lax
from jax.experimental import pallas as pl
from jax.experimental.pallas import tpu as pltpu
from jax.sharding import PartitionSpec as P

HEAD = 64
BLOCKS = 2
LANES = 128
CORES = 2

group_eps = 0.00064
norm_eps = 1e-06
key_eps = 1e-06
decay_scale = 0.606531
MESH = pl.DeviceIdType.MESH
F32 = jnp.float32
BF16 = jnp.bfloat16


def remote(src, dst, send, recv, axis, peer):
    return pltpu.make_async_remote_copy(
        src_ref=src,
        dst_ref=dst,
        send_sem=send,
        recv_sem=recv,
        device_id={axis: peer},
        device_id_type=MESH,
    )


def greet(peers):
    barrier = pltpu.get_barrier_semaphore()
    for axis, peer in peers:
        pl.semaphore_signal(barrier, inc=1, device_id={axis: peer}, device_id_type=MESH)
    pl.semaphore_wait(barrier, len(peers))


def grid_of(shape, dim):
    return lax.broadcasted_iota(jnp.int32, shape, dim)


def dot(a, b, dims=(((1,), (0,)), ((), ()))):
    return lax.dot_general(a.astype(BF16), b.astype(BF16), dims, preferred_element_type=F32)


def exact(a, b, dims=(((1,), (0,)), ((), ()))):
    return lax.dot_general(
        a, b, dims, preferred_element_type=F32, precision=lax.Precision.HIGHEST
    )


def split_dot(a, b):
    hi = a.astype(BF16)
    lo = (a - hi.astype(F32)).astype(BF16)
    return jnp.dot(hi, b, preferred_element_type=F32) + jnp.dot(lo, b, preferred_element_type=F32)


def split_right(a, b):
    hi = b.astype(BF16)
    lo = (b - hi.astype(F32)).astype(BF16)
    return jnp.dot(a, hi, preferred_element_type=F32) + jnp.dot(a, lo, preferred_element_type=F32)


def by_index(values, index):
    out = jnp.full(index.shape, values[0], jnp.int32)
    for i in range(1, len(values)):
        out = jnp.where(index == i, values[i], out)
    return out


def lane_sums(x):
    sq = x * x
    acc = sq[:, 0:LANES]
    for k in range(1, x.shape[1] // LANES):
        acc = acc + sq[:, k * LANES : (k + 1) * LANES]
    return acc


NT = (((1,), (1,)), ((), ()))
TN = (((0,), (0,)), ((), ()))


def mix(
    steps, block, projected, live, base, gain, state, final, span,
    vals_s, seen_s, read_s, ask_s, on_s,
):
    recept, keys, values, decay_pre, rate_pre, gate_pre = projected
    rows = recept.shape[0]
    held = rows // steps
    heads = span // HEAD
    tall = steps * heads
    seg = (grid_of((span, span), 0) // HEAD == grid_of((span, span), 1) // HEAD).astype(F32).astype(BF16)
    unit = keys * lax.rsqrt(split_dot(keys * keys, seg) + key_eps)
    removal = unit * jax.nn.sigmoid(rate_pre) * live
    logd = -decay_scale * jax.nn.sigmoid(decay_pre + base) * live
    step_of = grid_of((rows, 1), 0) % steps
    upto = logd
    shift = 1
    while shift < steps:
        upto = upto + jnp.where(step_of >= shift, pltpu.roll(upto, shift, 0), 0.0)
        shift *= 2
    grow = jnp.exp(upto)
    back = jnp.exp(-upto)
    u_in = unit * jnp.exp(upto - logd)
    q_in = recept * grow
    r_out = removal * back
    k_out = keys * live * back
    scale_out = gain * jax.nn.sigmoid(gate_pre) * live

    lane = grid_of((rows, LANES), 1)
    for j in range(span // LANES):
        pair = values[:, j * LANES : (j + 1) * LANES]
        vals_s[pl.ds(2 * j, rows, stride=heads), :] = pair
        vals_s[pl.ds(2 * j + 1, rows, stride=heads), :] = pltpu.roll(pair, HEAD, 1)

    if heads % 8 == 0:
        one = jnp.where(grid_of((heads, span), 0) == grid_of((heads, span), 1) // HEAD, 1.0, 0.0)

        def spread(a):
            return jnp.concatenate(
                [jnp.broadcast_to(a[s : s + 1], (heads, span)) * one for s in range(steps)], axis=0
            )
    else:
        pick = jnp.where(grid_of((tall, steps), 0) // heads == grid_of((tall, steps), 1), 1.0, 0.0)
        mask = jnp.where(grid_of((tall, span), 0) % heads == grid_of((tall, span), 1) // HEAD, 1.0, 0.0)

        def spread(a):
            return dot(pick, a) * mask

    pad = jnp.zeros((LANES - HEAD - 2 * steps, span), F32)
    ends = []
    for b in range(held):
        cut = slice(b * steps, (b + 1) * steps)
        ask_s[b, 0:tall, :] = spread(u_in[cut]).astype(BF16)
        ask_s[b, tall : 2 * tall, :] = spread(q_in[cut]).astype(BF16)
        ends.append(grow[(b + 1) * steps - 1 : (b + 1) * steps])
    for b in range(held):
        cut = slice(b * steps, (b + 1) * steps)
        against = jnp.concatenate([state[block, b], r_out[cut], k_out[cut], pad], axis=0)
        on_s[b] = dot(ask_s[b], against, NT)

    for b in range(held):
        first = b * tall
        vals = [vals_s[first + s * heads : first + (s + 1) * heads, :] for s in range(steps)]
        seen = []
        for s in range(steps):
            on = on_s[b, s * heads : (s + 1) * heads, :]
            acc = on
            for p in range(s):
                r = on[:, HEAD + p : HEAD + p + 1]
                k = on[:, HEAD + steps + p : HEAD + steps + p + 1]
                acc = acc + (k * vals[p] - r * seen[p])
            seen.append(acc)
            seen_s[first + s * heads : first + (s + 1) * heads, :] = acc
            on = on_s[b, tall + s * heads : tall + (s + 1) * heads, :]
            acc = on
            for p in range(s + 1):
                r = on[:, HEAD + p : HEAD + p + 1]
                k = on[:, HEAD + steps + p : HEAD + steps + p + 1]
                acc = acc + (k * vals[p] - r * seen[p])
            read_s[first + s * heads : first + (s + 1) * heads, :] = acc

    low = grid_of((held * tall, LANES), 1) < HEAD
    read = jnp.where(low, read_s[...], 0.0)
    mean = jnp.sum(read, axis=1, keepdims=True) / HEAD
    centered = jnp.where(low, read - mean, 0.0)
    var = jnp.sum(centered * centered, axis=1, keepdims=True) / HEAD
    read_s[...] = centered * lax.rsqrt(var + group_eps)
    flat = []
    for j in range(span // LANES):
        even = read_s[pl.ds(2 * j, rows, stride=heads), :]
        odd = read_s[pl.ds(2 * j + 1, rows, stride=heads), :]
        flat.append(jnp.where(lane < HEAD, even, pltpu.roll(odd, HEAD, 1)))
    gated = (jnp.concatenate(flat, axis=1) * scale_out).astype(BF16)

    def update():
        for b in range(held):
            cut = slice(b * steps, (b + 1) * steps)
            band = slice(b * tall, (b + 1) * tall)
            left = jnp.concatenate([vals_s[band, :], -seen_s[band, :]], axis=0)
            right = jnp.concatenate(
                [spread(k_out[cut] * ends[b]), spread(r_out[cut] * ends[b])], axis=0
            )
            final[block, b] = state[block, b] * ends[b] + dot(left, right, TN)[0:HEAD]

    return gated, update


def near_first(ntp):
    rows = [sorted(range(ntp), key=lambda g: (abs(g - t), g)) for t in range(ntp)]
    return [[rows[t][i] for t in range(ntp)] for i in range(ntp)]


def whole_kernel(
    ntp, ndp, steps, features, cap, share, lag,
    tokens, lengths, norm_gain, w0, w1, w2, w3, w4, w5, w_out, base_in, gain_in, states,
    out_ref, final_ref,
    xtok, lens, gains, bases, ogains, wbuf, wobuf, state,
    xg, xpk, xs, sqpk, sqd0, sqd1, acc0, acc1, packer, unpacker,
    part0, part1, recv_a0, recv_a1, send_b0, send_b1, recv_b0, recv_b1, tot0, tot1,
    gg, osend, orecv, psend, precv,
    vals_s, seen_s, read_s, ask_s, on_s,
    load_sem, wsem, xs_sem, xr_sem, ss_sem, sr_sem, as_sem, ar_sem, bs_sem, br_sem, ds_sem, dr_sem,
    qs_sem, qr_sem, gs_sem, gr_sem, os_sem, or_sem,
):
    weights = (w0, w1, w2, w3, w4, w5)
    depth = wbuf.shape[2]
    span = wobuf.shape[1]
    pieces, rows, wide = tot0.shape
    each = wide // span
    held = state.shape[1]
    seqs = xtok.shape[0]
    ratio = ntp // ndp
    here = seqs * steps
    every = ntp * cap
    packed = ntp * share
    nx = ndp // CORES
    count = ntp * pieces
    tp = lax.axis_index("tp")
    dp = lax.axis_index("dp")
    core = lax.rem(dp, CORES)
    xpos = dp // CORES
    partner = dp + 1 - 2 * core

    loads = [
        pltpu.make_async_copy(src, dst, load_sem.at[i])
        for i, (src, dst) in enumerate(
            (
                (tokens, xtok), (lengths, lens), (norm_gain, gains), (base_in, bases),
                (gain_in, ogains), (states, state), (w_out, wobuf),
            )
        )
    ]
    for cp in loads[:5]:
        cp.start()

    def load(block, c):
        return pltpu.make_async_copy(weights[c].at[block], wbuf.at[block, c], wsem.at[block, c])

    for c in range(6):
        load(0, c).start()
    loads[5].start()
    loads[6].start()
    for block in range(1, BLOCKS):
        for c in range(6):
            load(block, c).start()
    greet(
        [("tp", lax.rem(tp + k, ntp)) for k in range(1, ntp)]
        + [("dp", lax.rem(dp + k, ndp)) for k in range(1, ndp)]
    )
    for cp in loads[:2]:
        cp.wait()

    def spot(first, number):
        index = grid_of((number * steps, 1), 0)
        at, starts, counts = jnp.int32(0), [], []
        for b in range(number):
            if b % seqs == 0:
                at = jnp.int32(b // seqs * cap)
            starts.append(at)
            counts.append(lens[first + b])
            at = at + counts[-1]
        step = index % steps
        place = by_index(starts, index // steps) + step
        alive = step < by_index(counts, index // steps)
        shape = (number * steps, number // seqs * cap)
        one = jnp.where((place == grid_of(shape, 1)) & alive, 1.0, 0.0)
        return one, jnp.where(alive, 1.0, 0.0)

    mine, mine_live = spot(tp * seqs, seqs)
    mine = mine.astype(BF16)
    flat_tokens = xtok[...].reshape(here, depth)
    xg[tp] = dot(mine, flat_tokens, TN).astype(BF16)
    sends = []

    order = near_first(ntp)

    def source(i):
        at = order[0][0] * 0
        for k in range(ntp):
            here_k = order[k][ntp - 1]
            for t in range(ntp - 1):
                here_k = jnp.where(tp == t, order[k][t], here_k)
            at = jnp.where(i == k, here_k, at)
        return at

    def spread_out(buf, send, recv):
        for k in range(1, ntp):
            peer = source(k)
            cp = remote(buf.at[tp], buf.at[tp], send.at[k], recv.at[tp], "tp", peer)
            cp.start()
            sends.append(cp)

    def arrived(buf, send, recv, g):
        remote(buf.at[g], buf.at[g], send.at[0], recv.at[g], "tp", g).wait_recv()

    spread_out(xg, xs_sem.at[0], xr_sem.at[0])

    own_spot, live = spot(dp * held, held)
    own_spot = own_spot.astype(BF16)
    starts, counts, at = [], [], jnp.int32(0)
    for g in range(ntp):
        starts.append(at)
        number = jnp.int32(0)
        for b in range(seqs):
            number = number + lens[g * seqs + b]
        counts.append(number)
        at = at + number

    def ranks(index):
        return jnp.where(
            index % cap < by_index(counts, index // cap),
            by_index(starts, index // cap) + index % cap,
            -1,
        )

    packer[...] = jnp.where(
        grid_of((packed, every), 0) == ranks(grid_of((1, every), 1)), 1.0, 0.0
    ).astype(BF16)
    unpacker[...] = jnp.where(
        ranks(grid_of((every, 1), 0)) == grid_of((every, packed), 1), 1.0, 0.0
    ).astype(BF16)
    acc1[...] = jnp.zeros_like(acc1)
    ones = jnp.ones((8, LANES), F32)
    for cp in loads[2:5]:
        cp.wait()
    mine_packed = pl.ds(pl.multiple_of(tp * share, share), share)
    own_groups = pl.ds(pl.multiple_of(dp * rows, rows), rows)
    current = None

    for block in range(BLOCKS):
        first_block = block == 0
        size = cap if first_block else share
        half = size // CORES
        part, recv_a, send_b, recv_b, tot, sqd = (
            (part0, recv_a0, send_b0, recv_b0, tot0, sqd0)
            if first_block
            else (part1, recv_a1, send_b1, recv_b1, tot1, sqd1)
        )
        my_half = pl.ds(pl.multiple_of(core * half, half), half)
        other_half = pl.ds(pl.multiple_of((1 - core) * half, half), half)
        if not first_block:
            xpk[tp] = (current * gains[block : block + 1, :]).astype(BF16)
            spread_out(xpk, xs_sem.at[1], xr_sem.at[1])
            acc1[mine_packed, :] = lane_sums(current)
            sqpk[tp] = exact(ones, acc1[...], NT)
            spread_out(sqpk, ss_sem, sr_sem)

        def chip_of(g):
            return g // ratio // CORES

        def copy_a(g, j):
            return remote(
                part.at[g, j, other_half, :], recv_a.at[g, j],
                as_sem.at[block, g * pieces + j], ar_sem.at[block, g * pieces + j], "dp", partner,
            )

        def copy_b(g, j, peer, me):
            return remote(
                send_b.at[g, j], recv_b.at[me, g, j],
                bs_sem.at[block, peer, g * pieces + j], br_sem.at[block, me, g * pieces + j],
                "dp", CORES * peer + core,
            )

        def copy_d(g, j):
            base = g * size if not first_block else lax.rem(g, ratio) * size
            at = tot.at[j, pl.ds(pl.multiple_of(base + core * half, half), half), :]
            return remote(
                at, at, ds_sem.at[block, g * pieces + j], dr_sem.at[block, g * pieces + j],
                "dp", partner,
            )

        def expect_d(g, j):
            base = g * size if not first_block else lax.rem(g, ratio) * size
            at = tot.at[j, pl.ds(pl.multiple_of(base + (1 - core) * half, half), half), :]
            remote(
                at, at, ds_sem.at[block, g * pieces + j], dr_sem.at[block, g * pieces + j],
                "dp", partner,
            ).wait_recv()

        def stage_b(n):
            g, j = source(n // pieces), lax.rem(n, pieces)
            copy_a(g, j).wait_recv()
            total = part[g, j, my_half, :] + recv_a[g, j]
            part[g, j, my_half, :] = total
            send_b[g, j] = total.astype(BF16)
            for k in range(1, nx):
                peer = lax.rem(xpos + k, nx)
                if first_block:
                    @pl.when(chip_of(g) == peer)
                    def _():
                        copy_b(g, j, peer, xpos).start()
                else:
                    copy_b(g, j, peer, xpos).start()

        def stage_a(n, carry):
            g, j = source(n // pieces), lax.rem(n, pieces)

            @pl.when(j == 0)
            def _():
                @pl.when(n > 0)
                def _():
                    if first_block:
                        arrived(xg, xs_sem.at[0], xr_sem.at[0], g)
                    else:
                        arrived(xpk, xs_sem.at[1], xr_sem.at[1], g)

                if first_block:
                    x = xg[g].astype(F32)
                    xs[...] = (x * gains[0:1, :]).astype(BF16)
                    acc0[pl.ds(pl.multiple_of(g * cap, cap), cap), :] = lane_sums(x)

            @pl.when(n < pieces)
            def _():
                for c in range(each):
                    pltpu.make_async_copy(
                        wbuf.at[block, j * each + c], wbuf.at[block, j * each + c],
                        wsem.at[block, j * each + c],
                    ).wait()

            left = xs[...] if first_block else xpk[g]
            for c in range(each):
                part[g, j, :, c * span : (c + 1) * span] = jnp.dot(
                    left, wbuf[block, j * each + c], preferred_element_type=F32
                )
            copy_a(g, j).start()

            @pl.when(n >= lag)
            def _():
                stage_b(n - lag)

            return carry

        lax.fori_loop(0, count, stage_a, 0)
        if first_block:
            sqd[dp] = exact(ones, acc0[...], NT)
        else:
            for k in range(1, ntp):
                arrived(sqpk, ss_sem, sr_sem, source(k))
            sqd[dp] = jnp.sum(sqpk[...], axis=0)
        for k in range(1, ndp):
            cp = remote(
                sqd.at[dp], sqd.at[dp], qs_sem.at[block, k], qr_sem.at[block, k],
                "dp", lax.rem(dp + k, ndp),
            )
            cp.start()
            sends.append(cp)

        def late_b(n, carry):
            stage_b(n)
            return carry

        lax.fori_loop(count - lag, count, late_b, 0)

        def stage_c(n, carry):
            j = lax.rem(n, pieces)
            if first_block:
                q = n // pieces
                g = xpos * CORES * ratio + q
                base = lax.rem(q, ratio) * size
            else:
                g = source(n // pieces)
                base = g * size
            total = part[g, j, my_half, :]
            for k in range(1, nx):
                peer = lax.rem(xpos + k, nx)
                copy_b(g, j, peer, peer).wait_recv()
                total = total + recv_b[peer, g, j].astype(F32)
            at = pl.ds(pl.multiple_of(base + core * half, half), half)
            if first_block:
                @pl.when(q // ratio == core)
                def _():
                    tot[j, at, :] = total

                @pl.when(q // ratio != core)
                def _():
                    part[g, j, my_half, :] = total
                    remote(
                        part.at[g, j, my_half, :], tot.at[j, at, :],
                        ds_sem.at[block, g * pieces + j], dr_sem.at[block, g * pieces + j],
                        "dp", partner,
                    ).start()
            else:
                tot[j, at, :] = total
                copy_d(g, j).start()
            return carry

        lax.fori_loop(0, CORES * ratio * pieces if first_block else count, stage_c, 0)
        for k in range(1, ndp):
            src = lax.rem(dp + ndp - k, ndp)
            remote(
                sqd.at[src], sqd.at[src], qs_sem.at[block, k], qr_sem.at[block, k], "dp", src
            ).wait_recv()
        tall_index = rows if first_block else packed
        wide_index = every if first_block else packed
        begin = dp * rows if first_block else 0
        lanes = jnp.where(
            grid_of((tall_index, wide_index), 1) == grid_of((tall_index, wide_index), 0) + begin, 1.0, 0.0
        )
        inv = lax.rsqrt(exact(lanes, jnp.sum(sqd[...], axis=0), NT)[:, 0:1] / features + norm_eps)
        if first_block:
            to_own = own_spot
        else:
            to_own = dot(own_spot, unpacker[own_groups, :]).astype(BF16)
        if first_block:
            loads[5].wait()
            loads[6].wait()

        def expected(n, carry):
            g = dp * ratio + n // pieces if first_block else source(n // pieces)
            expect_d(g, lax.rem(n, pieces))
            return carry

        lax.fori_loop(0, ratio * pieces if first_block else count, expected, 0)

        def projected(i):
            cols = slice(i % each * span, (i % each + 1) * span)
            return split_right(to_own, tot[i // each, :, cols] * inv)

        gated, update = mix(
            steps, block, [projected(i) for i in range(6)],
            live, bases[block : block + 1, :], ogains[block : block + 1, :], state, final_ref, span,
            vals_s, seen_s, read_s, ask_s, on_s,
        )
        gg[block, dp] = dot(own_spot, gated, TN).astype(BF16)
        for k in range(1, ndp):
            cp = remote(
                gg.at[block, dp], gg.at[block, dp], gs_sem.at[block, k], gr_sem.at[block, k],
                "dp", lax.rem(dp + k, ndp),
            )
            cp.start()
            sends.append(cp)
        update()
        if first_block:
            current = dot(packer[mine_packed, :], xg[...].reshape(every, depth))
        else:
            back = dot(
                unpacker[pl.ds(pl.multiple_of(tp * cap, cap), cap), :],
                xpk[...].reshape(packed, depth),
            )
            current = back / gains[block : block + 1, :]

        def settle(n, carry):
            g, j = n // pieces, lax.rem(n, pieces)
            copy_a(g, j).wait_send()
            for k in range(1, nx):
                peer = lax.rem(xpos + k, nx)
                if first_block:
                    @pl.when(chip_of(g) == peer)
                    def _():
                        copy_b(g, j, peer, xpos).wait_send()
                else:
                    copy_b(g, j, peer, xpos).wait_send()
            if first_block:
                @pl.when(g // ratio == partner)
                def _():
                    copy_d(g, j).wait_send()
            else:
                copy_d(g, j).wait_send()
            return carry

        lax.fori_loop(0, count, settle, 0)
        for k in range(1, ndp):
            src = lax.rem(dp + ndp - k, ndp)
            remote(
                gg.at[block, src], gg.at[block, src], gs_sem.at[block, k], gr_sem.at[block, k], "dp", src
            ).wait_recv()
        rest = gg[block].reshape(every, span)
        if first_block:
            rest = dot(packer[...], rest).astype(BF16)
            sbuf, rbuf = psend, precv
        else:
            sbuf, rbuf = osend, orecv
        step_rows = sbuf.shape[1]
        partial = jnp.dot(rest, wobuf[block], preferred_element_type=F32)
        for g in range(ntp):
            sbuf[g] = partial[g * step_rows : (g + 1) * step_rows].astype(BF16)
        back_sends = []
        for k in range(1, ntp):
            peer = lax.rem(tp + k, ntp)
            cp = remote(
                sbuf.at[peer], rbuf.at[k], os_sem.at[block, k], or_sem.at[block, k], "tp", peer
            )
            cp.start()
            sends.append(cp)
            back_sends.append(cp)
        for g in range(ntp):
            current = current + jnp.where(
                tp == g, partial[g * step_rows : (g + 1) * step_rows], 0.0
            )
        for k in range(1, ntp):
            back_sends[k - 1].wait_recv()
            current = current + rbuf[k].astype(F32)
    result = jnp.where(
        mine_live > 0, exact(mine.astype(F32), current), flat_tokens.astype(F32)
    )
    out_ref[...] = result.reshape(out_ref.shape)
    for cp in sends:
        cp.wait_send()


def body(
    ntp, ndp,
    tokens, lengths, norm_gain,
    w_recept, w_key, w_value, w_decay, w_rate, w_gate,
    w_out, decay_base, out_gain, states,
):
    seqs, steps, depth = tokens.shape
    held = states.shape[1]
    live_rows = 7 * lengths.shape[0] // 2
    cap = seqs * steps
    share = 16 * -(-live_rows // (16 * ntp))
    rows = ntp // ndp * cap
    features = depth * ndp
    span = w_key.shape[2]
    pieces = 3
    lag = 3
    wide = 6 * span // pieces
    nx = ndp // CORES
    heads = span // HEAD
    tall = steps * heads
    every = ntp * cap
    packed = ntp * share
    count = ntp * pieces
    dma = pltpu.SemaphoreType.DMA
    vmem = pl.BlockSpec(memory_space=pltpu.VMEM)
    hbm = pl.BlockSpec(memory_space=pl.ANY)
    B = BLOCKS

    def buf(*shape, dtype=F32):
        return pltpu.VMEM(shape, dtype)

    return pl.pallas_call(
        functools.partial(whole_kernel, ntp, ndp, steps, features, cap, share, lag),
        out_shape=(
            jax.ShapeDtypeStruct((seqs, steps, depth), F32),
            jax.ShapeDtypeStruct(states.shape, F32),
        ),
        in_specs=[hbm] * 13,
        out_specs=(vmem, vmem),
        scratch_shapes=[
            buf(seqs, steps, depth, dtype=BF16),
            pltpu.SMEM(lengths.shape, jnp.int32),
            buf(B, depth), buf(B, span), buf(B, span),
            buf(B, 6, depth, span, dtype=BF16),
            buf(B, span, depth, dtype=BF16),
            buf(*states.shape),
            buf(ntp, cap, depth, dtype=BF16),
            buf(ntp, share, depth, dtype=BF16),
            buf(cap, depth, dtype=BF16),
            buf(ntp, 8, packed),
            buf(ndp, 8, every), buf(ndp, 8, packed),
            buf(every, LANES), buf(packed, LANES),
            buf(packed, every, dtype=BF16), buf(every, packed, dtype=BF16),
            buf(ntp, pieces, cap, wide), buf(ntp, pieces, share, wide),
            buf(ntp, pieces, cap // CORES, wide), buf(ntp, pieces, share // CORES, wide),
            buf(ntp, pieces, cap // CORES, wide, dtype=BF16),
            buf(ntp, pieces, share // CORES, wide, dtype=BF16),
            buf(nx, ntp, pieces, cap // CORES, wide, dtype=BF16),
            buf(nx, ntp, pieces, share // CORES, wide, dtype=BF16),
            buf(pieces, rows, wide), buf(pieces, packed, wide),
            buf(B, ndp, rows, span, dtype=BF16),
            buf(ntp, cap, depth, dtype=BF16),
            buf(ntp, cap, depth, dtype=BF16),
            buf(ntp, share, depth, dtype=BF16),
            buf(ntp, share, depth, dtype=BF16),
            buf(held * tall, LANES), buf(held * tall, LANES), buf(held * tall, LANES),
            buf(held, 2 * tall, span, dtype=BF16), buf(held, 2 * tall, LANES),
            dma((7,)), dma((B, 6)),
            dma((2, ntp)), dma((2, ntp)), dma((ntp,)), dma((ntp,)),
            dma((B, count)), dma((B, count)),
            dma((B, nx, count)), dma((B, nx, count)),
            dma((B, count)), dma((B, count)),
            dma((B, ndp)), dma((B, ndp)),
            dma((B, ndp)), dma((B, ndp)), dma((B, ntp)), dma((B, ntp)),
        ],
        compiler_params=pltpu.CompilerParams(
            collective_id=0, has_side_effects=True, vmem_limit_bytes=60 * 1024 * 1024
        ),
        name="whole",
    )(
        tokens, lengths, norm_gain,
        w_recept, w_key, w_value, w_decay, w_rate, w_gate,
        w_out, decay_base, out_gain, states,
    )


def solution(mesh):
    in_specs = (
        P(("grp", "tp"), None, "dp"),
        P("grp"),
        P(None, "dp"),
        P(None, "dp", "tp"),
        P(None, "dp", "tp"),
        P(None, "dp", "tp"),
        P(None, "dp", "tp"),
        P(None, "dp", "tp"),
        P(None, "dp", "tp"),
        P(None, "tp", "dp"),
        P(None, "tp"),
        P(None, "tp"),
        P(None, ("grp", "dp"), None, "tp"),
    )
    out_specs = (P(("grp", "tp"), None, "dp"), P(None, ("grp", "dp"), None, "tp"))
    run = functools.partial(body, mesh.shape["tp"], mesh.shape["dp"])
    return jax.shard_map(run, mesh=mesh, in_specs=in_specs, out_specs=out_specs, check_vma=False)
```

```python
import functools

import jax
import jax.numpy as jnp
from jax import lax
from jax.experimental import pallas as pl
from jax.experimental.pallas import tpu as pltpu
from jax.sharding import PartitionSpec as P

HEAD = 64
BLOCKS = 2
LANES = 128
CORES = 2

group_eps = 0.00064
norm_eps = 1e-06
key_eps = 1e-06
decay_scale = 0.606531
MESH = pl.DeviceIdType.MESH
F32 = jnp.float32
BF16 = jnp.bfloat16


def remote(src, dst, send, recv, axis, peer):
    return pltpu.make_async_remote_copy(
        src_ref=src,
        dst_ref=dst,
        send_sem=send,
        recv_sem=recv,
        device_id={axis: peer},
        device_id_type=MESH,
    )


def greet(peers):
    barrier = pltpu.get_barrier_semaphore()
    for axis, peer in peers:
        pl.semaphore_signal(barrier, inc=1, device_id={axis: peer}, device_id_type=MESH)
    pl.semaphore_wait(barrier, len(peers))


def grid_of(shape, dim):
    return lax.broadcasted_iota(jnp.int32, shape, dim)


def dot(a, b, dims=(((1,), (0,)), ((), ()))):
    return lax.dot_general(a.astype(BF16), b.astype(BF16), dims, preferred_element_type=F32)


def exact(a, b, dims=(((1,), (0,)), ((), ()))):
    return lax.dot_general(
        a, b, dims, preferred_element_type=F32, precision=lax.Precision.HIGHEST
    )


def split_dot(a, b):
    hi = a.astype(BF16)
    lo = (a - hi.astype(F32)).astype(BF16)
    return jnp.dot(hi, b, preferred_element_type=F32) + jnp.dot(lo, b, preferred_element_type=F32)


def split_right(a, b):
    hi = b.astype(BF16)
    lo = (b - hi.astype(F32)).astype(BF16)
    return jnp.dot(a, hi, preferred_element_type=F32) + jnp.dot(a, lo, preferred_element_type=F32)


def by_index(values, index):
    out = jnp.full(index.shape, values[0], jnp.int32)
    for i in range(1, len(values)):
        out = jnp.where(index == i, values[i], out)
    return out


def lane_sums(x):
    sq = x * x
    acc = sq[:, 0:LANES]
    for k in range(1, x.shape[1] // LANES):
        acc = acc + sq[:, k * LANES : (k + 1) * LANES]
    return acc


NT = (((1,), (1,)), ((), ()))
TN = (((0,), (0,)), ((), ()))


def mix(
    steps, block, begin, projected, live, base, gain, state, final, span,
    vals_s, seen_s, read_s, ask_s, on_s,
):
    recept, keys, values, decay_pre, rate_pre, gate_pre = projected
    rows = recept.shape[0]
    held = rows // steps
    heads = span // HEAD
    tall = steps * heads
    seg = (grid_of((span, span), 0) // HEAD == grid_of((span, span), 1) // HEAD).astype(F32).astype(BF16)
    unit = keys * lax.rsqrt(split_dot(keys * keys, seg) + key_eps)
    removal = unit * jax.nn.sigmoid(rate_pre) * live
    logd = -decay_scale * jax.nn.sigmoid(decay_pre + base) * live
    step_of = grid_of((rows, 1), 0) % steps
    upto = logd
    shift = 1
    while shift < steps:
        upto = upto + jnp.where(step_of >= shift, pltpu.roll(upto, shift, 0), 0.0)
        shift *= 2
    grow = jnp.exp(upto)
    back = jnp.exp(-upto)
    u_in = unit * jnp.exp(upto - logd)
    q_in = recept * grow
    r_out = removal * back
    k_out = keys * live * back
    scale_out = gain * jax.nn.sigmoid(gate_pre) * live

    lane = grid_of((rows, LANES), 1)
    for j in range(span // LANES):
        pair = values[:, j * LANES : (j + 1) * LANES]
        vals_s[pl.ds(2 * j, rows, stride=heads), :] = pair
        vals_s[pl.ds(2 * j + 1, rows, stride=heads), :] = pltpu.roll(pair, HEAD, 1)

    if heads % 8 == 0:
        one = jnp.where(grid_of((heads, span), 0) == grid_of((heads, span), 1) // HEAD, 1.0, 0.0)

        def spread(a):
            return jnp.concatenate(
                [jnp.broadcast_to(a[s : s + 1], (heads, span)) * one for s in range(steps)], axis=0
            )
    else:
        pick = jnp.where(grid_of((tall, steps), 0) // heads == grid_of((tall, steps), 1), 1.0, 0.0)
        mask = jnp.where(grid_of((tall, span), 0) % heads == grid_of((tall, span), 1) // HEAD, 1.0, 0.0)

        def spread(a):
            return dot(pick, a) * mask

    pad = jnp.zeros((LANES - HEAD - 2 * steps, span), F32)
    ends = []
    for b in range(held):
        cut = slice(b * steps, (b + 1) * steps)
        ask_s[b, 0:tall, :] = spread(u_in[cut]).astype(BF16)
        ask_s[b, tall : 2 * tall, :] = spread(q_in[cut]).astype(BF16)
        ends.append(grow[(b + 1) * steps - 1 : (b + 1) * steps])
    for b in range(held):
        cut = slice(b * steps, (b + 1) * steps)
        against = jnp.concatenate([state[block, begin + b], r_out[cut], k_out[cut], pad], axis=0)
        on_s[b] = dot(ask_s[b], against, NT)

    for b in range(held):
        first = b * tall
        vals = [vals_s[first + s * heads : first + (s + 1) * heads, :] for s in range(steps)]
        seen = []
        for s in range(steps):
            on = on_s[b, s * heads : (s + 1) * heads, :]
            acc = on
            for p in range(s):
                r = on[:, HEAD + p : HEAD + p + 1]
                k = on[:, HEAD + steps + p : HEAD + steps + p + 1]
                acc = acc + (k * vals[p] - r * seen[p])
            seen.append(acc)
            seen_s[first + s * heads : first + (s + 1) * heads, :] = acc
            on = on_s[b, tall + s * heads : tall + (s + 1) * heads, :]
            acc = on
            for p in range(s + 1):
                r = on[:, HEAD + p : HEAD + p + 1]
                k = on[:, HEAD + steps + p : HEAD + steps + p + 1]
                acc = acc + (k * vals[p] - r * seen[p])
            read_s[first + s * heads : first + (s + 1) * heads, :] = acc

    low = grid_of((held * tall, LANES), 1) < HEAD
    read = jnp.where(low, read_s[...], 0.0)
    mean = jnp.sum(read, axis=1, keepdims=True) / HEAD
    centered = jnp.where(low, read - mean, 0.0)
    var = jnp.sum(centered * centered, axis=1, keepdims=True) / HEAD
    read_s[...] = centered * lax.rsqrt(var + group_eps)
    flat = []
    for j in range(span // LANES):
        even = read_s[pl.ds(2 * j, rows, stride=heads), :]
        odd = read_s[pl.ds(2 * j + 1, rows, stride=heads), :]
        flat.append(jnp.where(lane < HEAD, even, pltpu.roll(odd, HEAD, 1)))
    gated = (jnp.concatenate(flat, axis=1) * scale_out).astype(BF16)

    def update():
        for b in range(held):
            cut = slice(b * steps, (b + 1) * steps)
            band = slice(b * tall, (b + 1) * tall)
            left = jnp.concatenate([vals_s[band, :], -seen_s[band, :]], axis=0)
            right = jnp.concatenate(
                [spread(k_out[cut] * ends[b]), spread(r_out[cut] * ends[b])], axis=0
            )
            final[block, begin + b] = state[block, begin + b] * ends[b] + dot(left, right, TN)[0:HEAD]

    return gated, update


def near_first(ntp):
    rows = [sorted(range(ntp), key=lambda g: (abs(g - t), g)) for t in range(ntp)]
    return [[rows[t][i] for t in range(ntp)] for i in range(ntp)]


def whole_kernel(
    ntp, ndp, steps, features, cap, share, lag, halves,
    tokens, lengths, norm_gain, w0, w1, w2, w3, w4, w5, w_out, base_in, gain_in, states,
    out_ref, final_ref,
    lens, gains, bases, ogains, wbuf, wobuf, state,
    xg, xpk, xs, sqpk, sqd0, sqd1, acc0, acc1, packer, unpacker,
    part0, part1, recv_a0, recv_a1, send_b0, send_b1, recv_b0, recv_b1, tot0, tot1,
    gg, osend, orecv, psend, precv,
    vals_s, seen_s, read_s, ask_s, on_s,
    load_sem, wsem, xs_sem, xr_sem, ss_sem, sr_sem, as_sem, ar_sem, bs_sem, br_sem, ds_sem, dr_sem,
    qs_sem, qr_sem, gs_sem, gr_sem, os_sem, or_sem,
):
    weights = (w0, w1, w2, w3, w4, w5)
    depth = wbuf.shape[2]
    span = wobuf.shape[1]
    pieces, rows, wide = tot0.shape
    each = wide // span
    held = state.shape[1]
    ratio = ntp // ndp
    seqs = cap // steps
    every = ntp * cap
    packed = ntp * share
    nx = ndp // CORES
    count = ntp * pieces
    tp = lax.axis_index("tp")
    dp = lax.axis_index("dp")
    core = lax.rem(dp, CORES)
    xpos = dp // CORES
    partner = dp + 1 - 2 * core

    loads = [
        pltpu.make_async_copy(src, dst, load_sem.at[i])
        for i, (src, dst) in enumerate(
            (
                (tokens, xg.at[tp]), (lengths, lens), (norm_gain, gains), (base_in, bases),
                (gain_in, ogains), (states, state), (w_out, wobuf),
            )
        )
    ]
    for cp in loads[:5]:
        cp.start()

    def load(block, c):
        return pltpu.make_async_copy(weights[c].at[block], wbuf.at[block, c], wsem.at[block, c])

    for c in range(6):
        load(0, c).start()
    loads[5].start()
    loads[6].start()
    for block in range(1, BLOCKS):
        for c in range(6):
            load(block, c).start()
    greet(
        [("tp", lax.rem(tp + k, ntp)) for k in range(1, ntp)]
        + [("dp", lax.rem(dp + k, ndp)) for k in range(1, ndp)]
    )
    for cp in loads[:2]:
        cp.wait()
    sends = []

    order = near_first(ntp)

    def source(i):
        at = order[0][0] * 0
        for k in range(ntp):
            here_k = order[k][ntp - 1]
            for t in range(ntp - 1):
                here_k = jnp.where(tp == t, order[k][t], here_k)
            at = jnp.where(i == k, here_k, at)
        return at

    def spread_out(buf, send, recv):
        for k in range(1, ntp):
            peer = source(k)
            cp = remote(buf.at[tp], buf.at[tp], send.at[k], recv.at[tp], "tp", peer)
            cp.start()
            sends.append(cp)

    def arrived(buf, send, recv, g):
        remote(buf.at[g], buf.at[g], send.at[0], recv.at[g], "tp", g).wait_recv()

    spread_out(xg, xs_sem.at[0], xr_sem.at[0])

    def alive(first, number, rows_here):
        index = grid_of((rows_here, 1), 0)
        return index % steps < by_index([lens[first + b] for b in range(number)], index // steps)

    live = jnp.where(alive(dp * held, held, rows), 1.0, 0.0)
    starts, counts, at = [], [], jnp.int32(0)
    for b in range(ntp * seqs):
        starts.append(at)
        counts.append(lens[b])
        at = at + counts[-1]

    def ranks(index):
        step = index % steps
        return jnp.where(
            step < by_index(counts, index // steps), by_index(starts, index // steps) + step, -1
        )

    for h in range(halves):
        column = grid_of((1, every // halves), 1)
        natural = column // (cap // halves) * cap + h * (cap // halves) + column % (cap // halves)
        packer[h] = jnp.where(
            grid_of((packed, every // halves), 0) == ranks(natural), 1.0, 0.0
        ).astype(BF16)
    still = alive(tp * seqs, seqs, cap)
    unpacker[...] = jnp.where(
        ranks(grid_of((every, 1), 0)) == grid_of((every, packed), 1), 1.0, 0.0
    ).astype(BF16)
    acc1[...] = jnp.zeros_like(acc1)
    ones = jnp.ones((8, LANES), F32)
    for cp in loads[2:5]:
        cp.wait()
    thin = cap // halves
    mine_packed = pl.ds(pl.multiple_of(tp * share, share), share)
    own_groups = pl.ds(pl.multiple_of(dp * rows, rows), rows)
    current = None

    for block in range(BLOCKS):
        first_block = block == 0
        size = cap if first_block else share
        half = size // CORES
        part, recv_a, send_b, recv_b, tot, sqd = (
            (part0, recv_a0, send_b0, recv_b0, tot0, sqd0)
            if first_block
            else (part1, recv_a1, send_b1, recv_b1, tot1, sqd1)
        )
        my_half = pl.ds(pl.multiple_of(core * half, half), half)
        other_half = pl.ds(pl.multiple_of((1 - core) * half, half), half)
        if not first_block:
            xpk[tp] = (current * gains[block : block + 1, :]).astype(BF16)
            spread_out(xpk, xs_sem.at[1], xr_sem.at[1])
            acc1[mine_packed, :] = lane_sums(current)
            sqpk[tp] = exact(ones, acc1[...], NT)
            spread_out(sqpk, ss_sem, sr_sem)

        def chip_of(g):
            return g // ratio // CORES

        def copy_a(g, j):
            return remote(
                part.at[g, j, other_half, :], recv_a.at[g, j],
                as_sem.at[block, g * pieces + j], ar_sem.at[block, g * pieces + j], "dp", partner,
            )

        def copy_b(g, j, peer, me):
            return remote(
                send_b.at[g, j], recv_b.at[me, g, j],
                bs_sem.at[block, peer, g * pieces + j], br_sem.at[block, me, g * pieces + j],
                "dp", CORES * peer + core,
            )

        def copy_d(g, j):
            base = g * size if not first_block else lax.rem(g, ratio) * size
            at = tot.at[j, pl.ds(pl.multiple_of(base + core * half, half), half), :]
            return remote(
                at, at, ds_sem.at[block, g * pieces + j], dr_sem.at[block, g * pieces + j],
                "dp", partner,
            )

        def expect_d(g, j):
            base = g * size if not first_block else lax.rem(g, ratio) * size
            at = tot.at[j, pl.ds(pl.multiple_of(base + (1 - core) * half, half), half), :]
            remote(
                at, at, ds_sem.at[block, g * pieces + j], dr_sem.at[block, g * pieces + j],
                "dp", partner,
            ).wait_recv()

        def stage_b(n):
            g, j = source(n // pieces), lax.rem(n, pieces)
            copy_a(g, j).wait_recv()
            total = part[g, j, my_half, :] + recv_a[g, j]
            part[g, j, my_half, :] = total
            send_b[g, j] = total.astype(BF16)
            for k in range(1, nx):
                peer = lax.rem(xpos + k, nx)
                if first_block:
                    @pl.when(chip_of(g) == peer)
                    def _():
                        copy_b(g, j, peer, xpos).start()
                else:
                    copy_b(g, j, peer, xpos).start()

        def stage_a(n, carry):
            g, j = source(n // pieces), lax.rem(n, pieces)

            @pl.when(j == 0)
            def _():
                @pl.when(n > 0)
                def _():
                    if first_block:
                        arrived(xg, xs_sem.at[0], xr_sem.at[0], g)
                    else:
                        arrived(xpk, xs_sem.at[1], xr_sem.at[1], g)

                if first_block:
                    x = xg[g].astype(F32)
                    xs[...] = (x * gains[0:1, :]).astype(BF16)
                    acc0[pl.ds(pl.multiple_of(g * cap, cap), cap), :] = lane_sums(x)

            @pl.when(n < pieces)
            def _():
                for c in range(each):
                    pltpu.make_async_copy(
                        wbuf.at[block, j * each + c], wbuf.at[block, j * each + c],
                        wsem.at[block, j * each + c],
                    ).wait()

            left = xs[...] if first_block else xpk[g]
            for c in range(each):
                part[g, j, :, c * span : (c + 1) * span] = jnp.dot(
                    left, wbuf[block, j * each + c], preferred_element_type=F32
                )
            copy_a(g, j).start()

            @pl.when(n >= lag)
            def _():
                stage_b(n - lag)

            return carry

        lax.fori_loop(0, count, stage_a, 0)
        if first_block:
            sqd[dp] = exact(ones, acc0[...], NT)
        else:
            for k in range(1, ntp):
                arrived(sqpk, ss_sem, sr_sem, source(k))
            sqd[dp] = jnp.sum(sqpk[...], axis=0)
        for k in range(1, ndp):
            cp = remote(
                sqd.at[dp], sqd.at[dp], qs_sem.at[block, k], qr_sem.at[block, k],
                "dp", lax.rem(dp + k, ndp),
            )
            cp.start()
            sends.append(cp)

        def late_b(n, carry):
            stage_b(n)
            return carry

        lax.fori_loop(count - lag, count, late_b, 0)

        def stage_c(n, carry):
            j = lax.rem(n, pieces)
            if first_block:
                q = n // pieces
                g = xpos * CORES * ratio + q
                base = lax.rem(q, ratio) * size
            else:
                g = source(n // pieces)
                base = g * size
            total = part[g, j, my_half, :]
            for k in range(1, nx):
                peer = lax.rem(xpos + k, nx)
                copy_b(g, j, peer, peer).wait_recv()
                total = total + recv_b[peer, g, j].astype(F32)
            at = pl.ds(pl.multiple_of(base + core * half, half), half)
            if first_block:
                @pl.when(q // ratio == core)
                def _():
                    tot[j, at, :] = total

                @pl.when(q // ratio != core)
                def _():
                    part[g, j, my_half, :] = total
                    remote(
                        part.at[g, j, my_half, :], tot.at[j, at, :],
                        ds_sem.at[block, g * pieces + j], dr_sem.at[block, g * pieces + j],
                        "dp", partner,
                    ).start()
            else:
                tot[j, at, :] = total
                copy_d(g, j).start()
            return carry

        lax.fori_loop(0, CORES * ratio * pieces if first_block else count, stage_c, 0)
        for k in range(1, ndp):
            src = lax.rem(dp + ndp - k, ndp)
            remote(
                sqd.at[src], sqd.at[src], qs_sem.at[block, k], qr_sem.at[block, k], "dp", src
            ).wait_recv()
        tall_index = rows if first_block else packed
        wide_index = every if first_block else packed
        begin = dp * rows if first_block else 0
        lanes = jnp.where(
            grid_of((tall_index, wide_index), 1) == grid_of((tall_index, wide_index), 0) + begin, 1.0, 0.0
        )
        inv = lax.rsqrt(exact(lanes, jnp.sum(sqd[...], axis=0), NT)[:, 0:1] / features + norm_eps)
        if first_block:
            loads[5].wait()
            loads[6].wait()

        def expected(n, carry):
            g = dp * ratio + n // pieces if first_block else source(n // pieces)
            expect_d(g, lax.rem(n, pieces))
            return carry

        lax.fori_loop(0, ratio * pieces if first_block else count, expected, 0)

        def projected(i, band):
            cols = slice(i % each * span, (i % each + 1) * span)
            if first_block:
                return tot[i // each, band, cols] * inv[band]
            take = pl.ds(pl.multiple_of(dp * rows + band.start, band.stop - band.start), band.stop - band.start)
            return split_right(unpacker[take, :], tot[i // each, :, cols] * inv)

        def share_out(h, k, peer, at):
            return remote(
                gg.at[block, h, at], gg.at[block, h, at], gs_sem.at[block, h, k], gr_sem.at[block, h, k],
                "dp", peer,
            )

        updates = []
        for h in range(halves):
            band = slice(h * rows // halves, (h + 1) * rows // halves)
            gated, update = mix(
                steps, block, h * held // halves, [projected(i, band) for i in range(6)],
                live[band], bases[block : block + 1, :], ogains[block : block + 1, :],
                state, final_ref, span,
                vals_s.at[h], seen_s.at[h], read_s.at[h], ask_s.at[h], on_s.at[h],
            )
            updates.append(update)
            gg[block, h, dp] = gated
            for k in range(1, ndp):
                cp = share_out(h, k, lax.rem(dp + k, ndp), dp)
                cp.start()
                sends.append(cp)
        for update in updates:
            update()
        if first_block:
            current = 0.0
            for h in range(halves):
                rows_h = xg[:, h * thin : (h + 1) * thin, :].reshape(every // halves, depth)
                current = current + dot(packer[h, mine_packed, :], rows_h)
        else:
            back = dot(
                unpacker[pl.ds(pl.multiple_of(tp * cap, cap), cap), :],
                xpk[...].reshape(packed, depth),
            )
            current = back / gains[block : block + 1, :]

        def settle(n, carry):
            g, j = n // pieces, lax.rem(n, pieces)
            copy_a(g, j).wait_send()
            for k in range(1, nx):
                peer = lax.rem(xpos + k, nx)
                if first_block:
                    @pl.when(chip_of(g) == peer)
                    def _():
                        copy_b(g, j, peer, xpos).wait_send()
                else:
                    copy_b(g, j, peer, xpos).wait_send()
            if first_block:
                @pl.when(g // ratio == partner)
                def _():
                    copy_d(g, j).wait_send()
            else:
                copy_d(g, j).wait_send()
            return carry

        lax.fori_loop(0, count, settle, 0)
        def shared(h):
            for k in range(1, ndp):
                src = lax.rem(dp + ndp - k, ndp)
                share_out(h, k, src, src).wait_recv()

        def give(h, left, sbuf, rbuf):
            partial = jnp.dot(left, wobuf[block], preferred_element_type=F32)
            many = partial.shape[0] // ntp
            for g in range(ntp):
                sbuf[h, g] = partial[g * many : (g + 1) * many].astype(BF16)
            started = []
            for k in range(1, ntp):
                peer = lax.rem(tp + k, ntp)
                cp = remote(
                    sbuf.at[h, peer], rbuf.at[h, k],
                    os_sem.at[block, h, k], or_sem.at[block, h, k], "tp", peer,
                )
                cp.start()
                started.append(cp)
            sends.extend(started)
            own = jnp.zeros((many, depth), F32)
            for g in range(ntp):
                own = own + jnp.where(tp == g, partial[g * many : (g + 1) * many], 0.0)
            return own, started

        if first_block:
            for h in range(halves):
                shared(h)
            left = 0.0
            for h in range(halves):
                left = left + dot(packer[h], gg[block, h].reshape(every // halves, span))
            own, started = give(0, left.astype(BF16), psend, precv)
            current = current + own
            for k in range(1, ntp):
                started[k - 1].wait_recv()
                current = current + precv[0, k].astype(F32)
        else:
            given = []
            for h in range(halves):
                shared(h)
                given.append(give(h, gg[block, h].reshape(every // halves, span), osend, orecv))
            for h in range(halves):
                own, started = given[h]
                cut = slice(h * thin, (h + 1) * thin)
                total = current[cut] + own
                for k in range(1, ntp):
                    started[k - 1].wait_recv()
                    total = total + orecv[h, k].astype(F32)
                out_ref[cut, :] = jnp.where(still[cut], total, xg[tp, cut, :].astype(F32))
    for cp in sends:
        cp.wait_send()


def body(
    ntp, ndp,
    tokens, lengths, norm_gain,
    w_recept, w_key, w_value, w_decay, w_rate, w_gate,
    w_out, decay_base, out_gain, states,
):
    seqs, steps, depth = tokens.shape
    held = states.shape[1]
    live_rows = 7 * lengths.shape[0] // 2
    cap = seqs * steps
    share = 16 * -(-live_rows // (16 * ntp))
    rows = ntp // ndp * cap
    features = depth * ndp
    span = w_key.shape[2]
    pieces = 2
    lag = 1
    halves = 2 if ntp == ndp and held % 2 == 0 else 1
    wide = 6 * span // pieces
    nx = ndp // CORES
    heads = span // HEAD
    tall = steps * heads
    every = ntp * cap
    packed = ntp * share
    count = ntp * pieces
    dma = pltpu.SemaphoreType.DMA
    vmem = pl.BlockSpec(memory_space=pltpu.VMEM)
    hbm = pl.BlockSpec(memory_space=pl.ANY)
    B = BLOCKS

    def buf(*shape, dtype=F32):
        return pltpu.VMEM(shape, dtype)

    stream, finals = pl.pallas_call(
        functools.partial(whole_kernel, ntp, ndp, steps, features, cap, share, lag, halves),
        out_shape=(
            pltpu.VMEM((cap, depth), F32),
            pltpu.VMEM(states.shape, F32),
        ),
        in_specs=[hbm] * 13,
        out_specs=(vmem, vmem),
        scratch_shapes=[
            pltpu.SMEM(lengths.shape, jnp.int32),
            buf(B, depth), buf(B, span), buf(B, span),
            buf(B, 6, depth, span, dtype=BF16),
            buf(B, span, depth, dtype=BF16),
            buf(*states.shape),
            buf(ntp, cap, depth, dtype=BF16),
            buf(ntp, share, depth, dtype=BF16),
            buf(cap, depth, dtype=BF16),
            buf(ntp, 8, packed),
            buf(ndp, 8, every), buf(ndp, 8, packed),
            buf(every, LANES), buf(packed, LANES),
            buf(halves, packed, every // halves, dtype=BF16), buf(every, packed, dtype=BF16),
            buf(ntp, pieces, cap, wide), buf(ntp, pieces, share, wide),
            buf(ntp, pieces, cap // CORES, wide), buf(ntp, pieces, share // CORES, wide),
            buf(ntp, pieces, cap // CORES, wide, dtype=BF16),
            buf(ntp, pieces, share // CORES, wide, dtype=BF16),
            buf(nx, ntp, pieces, cap // CORES, wide, dtype=BF16),
            buf(nx, ntp, pieces, share // CORES, wide, dtype=BF16),
            buf(pieces, rows, wide), buf(pieces, packed, wide),
            buf(B, halves, ndp, rows // halves, span, dtype=BF16),
            buf(halves, ntp, cap // halves, depth, dtype=BF16),
            buf(halves, ntp, cap // halves, depth, dtype=BF16),
            buf(1, ntp, share, depth, dtype=BF16),
            buf(1, ntp, share, depth, dtype=BF16),
            buf(halves, held * tall // halves, LANES),
            buf(halves, held * tall // halves, LANES),
            buf(halves, held * tall // halves, LANES),
            buf(halves, held // halves, 2 * tall, span, dtype=BF16),
            buf(halves, held // halves, 2 * tall, LANES),
            dma((7,)), dma((B, 6)),
            dma((2, ntp)), dma((2, ntp)), dma((ntp,)), dma((ntp,)),
            dma((B, count)), dma((B, count)),
            dma((B, nx, count)), dma((B, nx, count)),
            dma((B, count)), dma((B, count)),
            dma((B, ndp)), dma((B, ndp)),
            dma((B, halves, ndp)), dma((B, halves, ndp)), dma((B, halves, ntp)), dma((B, halves, ntp)),
        ],
        compiler_params=pltpu.CompilerParams(
            collective_id=0, has_side_effects=True, vmem_limit_bytes=56 * 1024 * 1024
        ),
        name="whole",
    )(
        *(
            pltpu.with_memory_space_constraint(a, pltpu.HBM)
            for a in (
                tokens.reshape(cap, depth), lengths, norm_gain,
                w_recept, w_key, w_value, w_decay, w_rate, w_gate,
                w_out, decay_base, out_gain, states,
            )
        )
    )
    return stream.reshape(tokens.shape), finals


def solution(mesh):
    in_specs = (
        P(("grp", "tp"), None, "dp"),
        P("grp"),
        P(None, "dp"),
        P(None, "dp", "tp"),
        P(None, "dp", "tp"),
        P(None, "dp", "tp"),
        P(None, "dp", "tp"),
        P(None, "dp", "tp"),
        P(None, "dp", "tp"),
        P(None, "tp", "dp"),
        P(None, "tp"),
        P(None, "tp"),
        P(None, ("grp", "dp"), None, "tp"),
    )
    out_specs = (P(("grp", "tp"), None, "dp"), P(None, ("grp", "dp"), None, "tp"))
    run = functools.partial(body, mesh.shape["tp"], mesh.shape["dp"])
    return jax.shard_map(run, mesh=mesh, in_specs=in_specs, out_specs=out_specs, check_vma=False)
```

```python
import functools

import jax
import jax.numpy as jnp
from jax import lax
from jax.experimental import pallas as pl
from jax.experimental.pallas import tpu as pltpu
from jax.sharding import PartitionSpec as P

HEAD = 64
BLOCKS = 2
LANES = 128
CORES = 2

group_eps = 0.00064
norm_eps = 1e-06
key_eps = 1e-06
decay_scale = 0.606531
MESH = pl.DeviceIdType.MESH
F32 = jnp.float32
BF16 = jnp.bfloat16


def remote(src, dst, send, recv, axis, peer):
    return pltpu.make_async_remote_copy(
        src_ref=src,
        dst_ref=dst,
        send_sem=send,
        recv_sem=recv,
        device_id={axis: peer},
        device_id_type=MESH,
    )


def greet(peers):
    barrier = pltpu.get_barrier_semaphore()
    for axis, peer in peers:
        pl.semaphore_signal(barrier, inc=1, device_id={axis: peer}, device_id_type=MESH)
    pl.semaphore_wait(barrier, len(peers))


def grid_of(shape, dim):
    return lax.broadcasted_iota(jnp.int32, shape, dim)


def dot(a, b, dims=(((1,), (0,)), ((), ()))):
    return lax.dot_general(a.astype(BF16), b.astype(BF16), dims, preferred_element_type=F32)


def exact(a, b, dims=(((1,), (0,)), ((), ()))):
    return lax.dot_general(
        a, b, dims, preferred_element_type=F32, precision=lax.Precision.HIGHEST
    )


def split_dot(a, b):
    hi = a.astype(BF16)
    lo = (a - hi.astype(F32)).astype(BF16)
    return jnp.dot(hi, b, preferred_element_type=F32) + jnp.dot(lo, b, preferred_element_type=F32)


def split_right(a, b):
    hi = b.astype(BF16)
    lo = (b - hi.astype(F32)).astype(BF16)
    return jnp.dot(a, hi, preferred_element_type=F32) + jnp.dot(a, lo, preferred_element_type=F32)


def by_index(values, index):
    out = jnp.full(index.shape, values[0], jnp.int32)
    for i in range(1, len(values)):
        out = jnp.where(index == i, values[i], out)
    return out


def lane_sums(x):
    sq = x * x
    acc = sq[:, 0:LANES]
    for k in range(1, x.shape[1] // LANES):
        acc = acc + sq[:, k * LANES : (k + 1) * LANES]
    return acc


NT = (((1,), (1,)), ((), ()))
TN = (((0,), (0,)), ((), ()))


def mix(
    steps, block, begin, projected, live, base, gain, state, final, span,
    vals_s, seen_s, read_s, ask_s, on_s,
):
    recept, keys, values, decay_pre, rate_pre, gate_pre = projected
    rows = recept.shape[0]
    held = rows // steps
    heads = span // HEAD
    tall = steps * heads
    seg = (grid_of((span, span), 0) // HEAD == grid_of((span, span), 1) // HEAD).astype(F32).astype(BF16)
    unit = keys * lax.rsqrt(split_dot(keys * keys, seg) + key_eps)
    removal = unit * jax.nn.sigmoid(rate_pre) * live
    logd = -decay_scale * jax.nn.sigmoid(decay_pre + base) * live
    step_of = grid_of((rows, 1), 0) % steps
    upto = logd
    shift = 1
    while shift < steps:
        upto = upto + jnp.where(step_of >= shift, pltpu.roll(upto, shift, 0), 0.0)
        shift *= 2
    grow = jnp.exp(upto)
    back = jnp.exp(-upto)
    u_in = unit * jnp.exp(upto - logd)
    q_in = recept * grow
    r_out = removal * back
    k_out = keys * live * back
    scale_out = gain * jax.nn.sigmoid(gate_pre) * live

    lane = grid_of((rows, LANES), 1)
    for j in range(span // LANES):
        pair = values[:, j * LANES : (j + 1) * LANES]
        vals_s[pl.ds(2 * j, rows, stride=heads), :] = pair
        vals_s[pl.ds(2 * j + 1, rows, stride=heads), :] = pltpu.roll(pair, HEAD, 1)

    if heads % 8 == 0:
        one = jnp.where(grid_of((heads, span), 0) == grid_of((heads, span), 1) // HEAD, 1.0, 0.0)

        def spread(a):
            return jnp.concatenate(
                [jnp.broadcast_to(a[s : s + 1], (heads, span)) * one for s in range(steps)], axis=0
            )
    else:
        pick = jnp.where(grid_of((tall, steps), 0) // heads == grid_of((tall, steps), 1), 1.0, 0.0)
        mask = jnp.where(grid_of((tall, span), 0) % heads == grid_of((tall, span), 1) // HEAD, 1.0, 0.0)

        def spread(a):
            return dot(pick, a) * mask

    pad = jnp.zeros((LANES - HEAD - 2 * steps, span), F32)
    ends = []
    for b in range(held):
        cut = slice(b * steps, (b + 1) * steps)
        ask_s[b, 0:tall, :] = spread(u_in[cut]).astype(BF16)
        ask_s[b, tall : 2 * tall, :] = spread(q_in[cut]).astype(BF16)
        ends.append(grow[(b + 1) * steps - 1 : (b + 1) * steps])
    for b in range(held):
        cut = slice(b * steps, (b + 1) * steps)
        against = jnp.concatenate([state[block, begin + b], r_out[cut], k_out[cut], pad], axis=0)
        on_s[b] = dot(ask_s[b], against, NT)

    for b in range(held):
        first = b * tall
        vals = [vals_s[first + s * heads : first + (s + 1) * heads, :] for s in range(steps)]
        seen = []
        for s in range(steps):
            on = on_s[b, s * heads : (s + 1) * heads, :]
            acc = on
            for p in range(s):
                r = on[:, HEAD + p : HEAD + p + 1]
                k = on[:, HEAD + steps + p : HEAD + steps + p + 1]
                acc = acc + (k * vals[p] - r * seen[p])
            seen.append(acc)
            seen_s[first + s * heads : first + (s + 1) * heads, :] = acc
            on = on_s[b, tall + s * heads : tall + (s + 1) * heads, :]
            acc = on
            for p in range(s + 1):
                r = on[:, HEAD + p : HEAD + p + 1]
                k = on[:, HEAD + steps + p : HEAD + steps + p + 1]
                acc = acc + (k * vals[p] - r * seen[p])
            read_s[first + s * heads : first + (s + 1) * heads, :] = acc

    low = grid_of((held * tall, LANES), 1) < HEAD
    read = jnp.where(low, read_s[...], 0.0)
    mean = jnp.sum(read, axis=1, keepdims=True) / HEAD
    centered = jnp.where(low, read - mean, 0.0)
    var = jnp.sum(centered * centered, axis=1, keepdims=True) / HEAD
    read_s[...] = centered * lax.rsqrt(var + group_eps)
    flat = []
    for j in range(span // LANES):
        even = read_s[pl.ds(2 * j, rows, stride=heads), :]
        odd = read_s[pl.ds(2 * j + 1, rows, stride=heads), :]
        flat.append(jnp.where(lane < HEAD, even, pltpu.roll(odd, HEAD, 1)))
    gated = (jnp.concatenate(flat, axis=1) * scale_out).astype(BF16)

    def update():
        for b in range(held):
            cut = slice(b * steps, (b + 1) * steps)
            band = slice(b * tall, (b + 1) * tall)
            left = jnp.concatenate([vals_s[band, :], -seen_s[band, :]], axis=0)
            right = jnp.concatenate(
                [spread(k_out[cut] * ends[b]), spread(r_out[cut] * ends[b])], axis=0
            )
            final[block, begin + b] = state[block, begin + b] * ends[b] + dot(left, right, TN)[0:HEAD]

    return gated, update


def near_first(ntp):
    rows = [sorted(range(ntp), key=lambda g: (abs(g - t), g)) for t in range(ntp)]
    return [[rows[t][i] for t in range(ntp)] for i in range(ntp)]


def whole_kernel(
    ntp, ndp, steps, features, cap, share, live_rows, lag, halves,
    tokens, lengths, norm_gain, w0, w1, w2, w3, w4, w5, w_out, base_in, gain_in, states,
    out_ref, final_ref,
    lens, gains, bases, ogains, wbuf, wobuf, state,
    xg, xpk, xs, sqpk, sqd0, sqd1, acc0, acc1, packer, unpacker,
    part0, part1, recv_a0, recv_a1, send_b0, send_b1, recv_b0, recv_b1, tot0, tot1,
    gg, osend, orecv, psend, precv,
    vals_s, seen_s, read_s, ask_s, on_s,
    load_sem, wsem, xs_sem, xr_sem, ss_sem, sr_sem, as_sem, ar_sem, bs_sem, br_sem, ds_sem, dr_sem,
    qs_sem, qr_sem, gs_sem, gr_sem, os_sem, or_sem,
):
    weights = (w0, w1, w2, w3, w4, w5)
    depth = wbuf.shape[2]
    span = wobuf.shape[1]
    pieces, rows, wide = tot0.shape
    each = wide // span
    held = state.shape[1]
    ratio = ntp // ndp
    seqs = cap // steps
    every = ntp * cap
    packed = ntp * share
    nx = ndp // CORES
    count = ntp * pieces
    tp = lax.axis_index("tp")
    dp = lax.axis_index("dp")
    core = lax.rem(dp, CORES)
    xpos = dp // CORES
    partner = dp + 1 - 2 * core

    loads = [
        pltpu.make_async_copy(src, dst, load_sem.at[i])
        for i, (src, dst) in enumerate(
            (
                (tokens, xg.at[tp]), (lengths, lens), (norm_gain, gains), (base_in, bases),
                (gain_in, ogains), (states, state), (w_out, wobuf),
            )
        )
    ]
    for cp in loads[:5]:
        cp.start()

    def load(block, c):
        return pltpu.make_async_copy(weights[c].at[block], wbuf.at[block, c], wsem.at[block, c])

    for c in range(6):
        load(0, c).start()
    loads[5].start()
    loads[6].start()
    for block in range(1, BLOCKS):
        for c in range(6):
            load(block, c).start()
    greet(
        [("tp", lax.rem(tp + k, ntp)) for k in range(1, ntp)]
        + [("dp", lax.rem(dp + k, ndp)) for k in range(1, ndp)]
    )
    for cp in loads[:2]:
        cp.wait()
    sends = []

    order = near_first(ntp)

    def source(i):
        at = order[0][0] * 0
        for k in range(ntp):
            here_k = order[k][ntp - 1]
            for t in range(ntp - 1):
                here_k = jnp.where(tp == t, order[k][t], here_k)
            at = jnp.where(i == k, here_k, at)
        return at

    def spread_out(buf, send, recv):
        for k in range(1, ntp):
            peer = source(k)
            cp = remote(buf.at[tp], buf.at[tp], send.at[k], recv.at[tp], "tp", peer)
            cp.start()
            sends.append(cp)

    def arrived(buf, send, recv, g):
        remote(buf.at[g], buf.at[g], send.at[0], recv.at[g], "tp", g).wait_recv()

    spread_out(xg, xs_sem.at[0], xr_sem.at[0])

    def alive(first, number, rows_here):
        index = grid_of((rows_here, 1), 0)
        return index % steps < by_index([lens[first + b] for b in range(number)], index // steps)

    live = jnp.where(alive(dp * held, held, rows), 1.0, 0.0)
    starts, counts, at = [], [], jnp.int32(0)
    for b in range(ntp * seqs):
        starts.append(at)
        counts.append(lens[b])
        at = at + counts[-1]

    def ranks(index):
        step = index % steps
        return jnp.where(
            step < by_index(counts, index // steps), by_index(starts, index // steps) + step, -1
        )

    for h in range(halves):
        column = grid_of((1, every // halves), 1)
        natural = column // (cap // halves) * cap + h * (cap // halves) + column % (cap // halves)
        packer[h] = jnp.where(
            grid_of((packed, every // halves), 0) == ranks(natural), 1.0, 0.0
        ).astype(BF16)
    still = alive(tp * seqs, seqs, cap)
    unpacker[...] = jnp.where(
        ranks(grid_of((every, 1), 0)) == grid_of((every, packed), 1), 1.0, 0.0
    ).astype(BF16)
    acc1[...] = jnp.zeros_like(acc1)
    clear = -(-live_rows // (share // CORES)) * (share // CORES)
    if clear < packed:
        for j in range(pieces):
            tot1[j, clear:, :] = jnp.zeros((packed - clear, wide), F32)
    ones = jnp.ones((8, LANES), F32)
    for cp in loads[2:5]:
        cp.wait()
    thin = cap // halves
    mine_packed = pl.ds(pl.multiple_of(tp * share, share), share)
    own_groups = pl.ds(pl.multiple_of(dp * rows, rows), rows)
    current = None

    for block in range(BLOCKS):
        first_block = block == 0
        size = cap if first_block else share
        half = size // CORES
        part, recv_a, send_b, recv_b, tot, sqd = (
            (part0, recv_a0, send_b0, recv_b0, tot0, sqd0)
            if first_block
            else (part1, recv_a1, send_b1, recv_b1, tot1, sqd1)
        )
        my_half = pl.ds(pl.multiple_of(core * half, half), half)
        other_half = pl.ds(pl.multiple_of((1 - core) * half, half), half)
        if not first_block:
            xpk[tp] = (current * gains[block : block + 1, :]).astype(BF16)
            spread_out(xpk, xs_sem.at[1], xr_sem.at[1])
            acc1[mine_packed, :] = lane_sums(current)
            sqpk[tp] = exact(ones, acc1[...], NT)
            spread_out(sqpk, ss_sem, sr_sem)

        def chip_of(g):
            return g // ratio // CORES

        def copy_a(g, j):
            return remote(
                part.at[g, j, other_half, :], recv_a.at[g, j],
                as_sem.at[block, g * pieces + j], ar_sem.at[block, g * pieces + j], "dp", partner,
            )

        def copy_b(g, j, peer, me):
            return remote(
                send_b.at[g, j], recv_b.at[me, g, j],
                bs_sem.at[block, peer, g * pieces + j], br_sem.at[block, me, g * pieces + j],
                "dp", CORES * peer + core,
            )

        def copy_d(g, j):
            base = g * size if not first_block else lax.rem(g, ratio) * size
            at = tot.at[j, pl.ds(pl.multiple_of(base + core * half, half), half), :]
            return remote(
                at, at, ds_sem.at[block, g * pieces + j], dr_sem.at[block, g * pieces + j],
                "dp", partner,
            )

        def expect_d(g, j):
            base = g * size if not first_block else lax.rem(g, ratio) * size
            at = tot.at[j, pl.ds(pl.multiple_of(base + (1 - core) * half, half), half), :]
            remote(
                at, at, ds_sem.at[block, g * pieces + j], dr_sem.at[block, g * pieces + j],
                "dp", partner,
            ).wait_recv()

        def used(g, c):
            return first_block or g * size + c * half < live_rows

        def guarded(test, action):
            if test is True:
                action()
            else:
                pl.when(test)(action)

        def stage_b(n):
            guarded(used(source(n // pieces), core), lambda: combine(n))

        def combine(n):
            g, j = source(n // pieces), lax.rem(n, pieces)
            copy_a(g, j).wait_recv()
            total = part[g, j, my_half, :] + recv_a[g, j]
            part[g, j, my_half, :] = total
            send_b[g, j] = total.astype(BF16)
            for k in range(1, nx):
                peer = lax.rem(xpos + k, nx)
                if first_block:
                    @pl.when(chip_of(g) == peer)
                    def _():
                        copy_b(g, j, peer, xpos).start()
                else:
                    copy_b(g, j, peer, xpos).start()

        def stage_a(n, carry):
            g, j = source(n // pieces), lax.rem(n, pieces)

            @pl.when(j == 0)
            def _():
                @pl.when(n > 0)
                def _():
                    if first_block:
                        arrived(xg, xs_sem.at[0], xr_sem.at[0], g)
                    else:
                        arrived(xpk, xs_sem.at[1], xr_sem.at[1], g)

                if first_block:
                    x = xg[g].astype(F32)
                    xs[...] = (x * gains[0:1, :]).astype(BF16)
                    acc0[pl.ds(pl.multiple_of(g * cap, cap), cap), :] = lane_sums(x)

            @pl.when(n < pieces)
            def _():
                for c in range(each):
                    pltpu.make_async_copy(
                        wbuf.at[block, j * each + c], wbuf.at[block, j * each + c],
                        wsem.at[block, j * each + c],
                    ).wait()

            left = xs[...] if first_block else xpk[g]
            for c in range(each):
                part[g, j, :, c * span : (c + 1) * span] = jnp.dot(
                    left, wbuf[block, j * each + c], preferred_element_type=F32
                )
            guarded(used(g, 1 - core), lambda: copy_a(g, j).start())

            @pl.when(n >= lag)
            def _():
                stage_b(n - lag)

            return carry

        lax.fori_loop(0, count, stage_a, 0)
        def late_b(n, carry):
            stage_b(n)
            return carry

        lax.fori_loop(count - lag, count, late_b, 0)
        if first_block:
            sqd[dp] = exact(ones, acc0[...], NT)
        else:
            for k in range(1, ntp):
                arrived(sqpk, ss_sem, sr_sem, source(k))
            sqd[dp] = jnp.sum(sqpk[...], axis=0)
        for k in range(1, ndp):
            cp = remote(
                sqd.at[dp], sqd.at[dp], qs_sem.at[block, k], qr_sem.at[block, k],
                "dp", lax.rem(dp + k, ndp),
            )
            cp.start()
            sends.append(cp)

        def stage_c(n, carry):
            g = 0 if first_block else source(n // pieces)
            guarded(used(g, core), lambda: finish(n))
            return carry

        def finish(n):
            j = lax.rem(n, pieces)
            if first_block:
                q = n // pieces
                g = xpos * CORES * ratio + q
                base = lax.rem(q, ratio) * size
            else:
                g = source(n // pieces)
                base = g * size
            total = part[g, j, my_half, :]
            for k in range(1, nx):
                peer = lax.rem(xpos + k, nx)
                copy_b(g, j, peer, peer).wait_recv()
                total = total + recv_b[peer, g, j].astype(F32)
            at = pl.ds(pl.multiple_of(base + core * half, half), half)
            if first_block:
                @pl.when(q // ratio == core)
                def _():
                    tot[j, at, :] = total

                @pl.when(q // ratio != core)
                def _():
                    part[g, j, my_half, :] = total
                    remote(
                        part.at[g, j, my_half, :], tot.at[j, at, :],
                        ds_sem.at[block, g * pieces + j], dr_sem.at[block, g * pieces + j],
                        "dp", partner,
                    ).start()
            else:
                tot[j, at, :] = total
                copy_d(g, j).start()

        lax.fori_loop(0, CORES * ratio * pieces if first_block else count, stage_c, 0)
        for k in range(1, ndp):
            src = lax.rem(dp + ndp - k, ndp)
            remote(
                sqd.at[src], sqd.at[src], qs_sem.at[block, k], qr_sem.at[block, k], "dp", src
            ).wait_recv()
        tall_index = rows if first_block else packed
        wide_index = every if first_block else packed
        begin = dp * rows if first_block else 0
        lanes = jnp.where(
            grid_of((tall_index, wide_index), 1) == grid_of((tall_index, wide_index), 0) + begin, 1.0, 0.0
        )
        inv = lax.rsqrt(exact(lanes, jnp.sum(sqd[...], axis=0), NT)[:, 0:1] / features + norm_eps)
        if first_block:
            loads[5].wait()
            loads[6].wait()

        def expected(n, carry):
            g = dp * ratio + n // pieces if first_block else source(n // pieces)
            guarded(used(g, 1 - core), lambda: expect_d(g, lax.rem(n, pieces)))
            return carry

        lax.fori_loop(0, ratio * pieces if first_block else count, expected, 0)

        def projected(i, band):
            cols = slice(i % each * span, (i % each + 1) * span)
            if first_block:
                return tot[i // each, band, cols] * inv[band]
            take = pl.ds(pl.multiple_of(dp * rows + band.start, band.stop - band.start), band.stop - band.start)
            return split_right(unpacker[take, :], tot[i // each, :, cols] * inv)

        def share_out(h, k, peer, at):
            return remote(
                gg.at[block, h, at], gg.at[block, h, at], gs_sem.at[block, h, k], gr_sem.at[block, h, k],
                "dp", peer,
            )

        updates = []
        for h in range(halves):
            band = slice(h * rows // halves, (h + 1) * rows // halves)
            gated, update = mix(
                steps, block, h * held // halves, [projected(i, band) for i in range(6)],
                live[band], bases[block : block + 1, :], ogains[block : block + 1, :],
                state, final_ref, span,
                vals_s.at[h], seen_s.at[h], read_s.at[h], ask_s.at[h], on_s.at[h],
            )
            updates.append(update)
            gg[block, h, dp] = gated
            for k in range(1, ndp):
                cp = share_out(h, k, lax.rem(dp + k, ndp), dp)
                cp.start()
                sends.append(cp)
        for update in updates:
            update()
        if first_block:
            current = 0.0
            for h in range(halves):
                rows_h = xg[:, h * thin : (h + 1) * thin, :].reshape(every // halves, depth)
                current = current + dot(packer[h, mine_packed, :], rows_h)
        else:
            back = dot(
                unpacker[pl.ds(pl.multiple_of(tp * cap, cap), cap), :],
                xpk[...].reshape(packed, depth),
            )
            current = back / gains[block : block + 1, :]

        def settle(n, carry):
            g, j = n // pieces, lax.rem(n, pieces)
            guarded(used(g, 1 - core), lambda: copy_a(g, j).wait_send())

            def sent():
                for k in range(1, nx):
                    peer = lax.rem(xpos + k, nx)
                    if first_block:
                        @pl.when(chip_of(g) == peer)
                        def _():
                            copy_b(g, j, peer, xpos).wait_send()
                    else:
                        copy_b(g, j, peer, xpos).wait_send()
                if first_block:
                    @pl.when(g // ratio == partner)
                    def _():
                        copy_d(g, j).wait_send()
                else:
                    copy_d(g, j).wait_send()

            guarded(used(g, core), sent)
            return carry

        lax.fori_loop(0, count, settle, 0)
        def shared(h):
            for k in range(1, ndp):
                src = lax.rem(dp + ndp - k, ndp)
                share_out(h, k, src, src).wait_recv()

        def give(h, left, sbuf, rbuf):
            partial = jnp.dot(left, wobuf[block], preferred_element_type=F32)
            many = partial.shape[0] // ntp
            for g in range(ntp):
                sbuf[h, g] = partial[g * many : (g + 1) * many].astype(BF16)
            started = []
            for k in range(1, ntp):
                peer = lax.rem(tp + k, ntp)
                cp = remote(
                    sbuf.at[h, peer], rbuf.at[h, k],
                    os_sem.at[block, h, k], or_sem.at[block, h, k], "tp", peer,
                )
                cp.start()
                started.append(cp)
            sends.extend(started)
            own = jnp.zeros((many, depth), F32)
            for g in range(ntp):
                own = own + jnp.where(tp == g, partial[g * many : (g + 1) * many], 0.0)
            return own, started

        if first_block:
            for h in range(halves):
                shared(h)
            left = 0.0
            for h in range(halves):
                left = left + dot(packer[h], gg[block, h].reshape(every // halves, span))
            own, started = give(0, left.astype(BF16), psend, precv)
            current = current + own
            for k in range(1, ntp):
                started[k - 1].wait_recv()
                current = current + precv[0, k].astype(F32)
        else:
            given = []
            for h in range(halves):
                shared(h)
                given.append(give(h, gg[block, h].reshape(every // halves, span), osend, orecv))
            for h in range(halves):
                own, started = given[h]
                cut = slice(h * thin, (h + 1) * thin)
                total = current[cut] + own
                for k in range(1, ntp):
                    started[k - 1].wait_recv()
                    total = total + orecv[h, k].astype(F32)
                out_ref[cut, :] = jnp.where(still[cut], total, xg[tp, cut, :].astype(F32))
    for cp in sends:
        cp.wait_send()


def body(
    ntp, ndp,
    tokens, lengths, norm_gain,
    w_recept, w_key, w_value, w_decay, w_rate, w_gate,
    w_out, decay_base, out_gain, states,
):
    seqs, steps, depth = tokens.shape
    held = states.shape[1]
    live_rows = 7 * lengths.shape[0] // 2
    cap = seqs * steps
    share = 16 * -(-live_rows // (16 * ntp))
    rows = ntp // ndp * cap
    features = depth * ndp
    span = w_key.shape[2]
    pieces = 2
    lag = 1
    halves = 2 if ntp == ndp and held % 2 == 0 else 1
    wide = 6 * span // pieces
    nx = ndp // CORES
    heads = span // HEAD
    tall = steps * heads
    every = ntp * cap
    packed = ntp * share
    count = ntp * pieces
    dma = pltpu.SemaphoreType.DMA
    vmem = pl.BlockSpec(memory_space=pltpu.VMEM)
    hbm = pl.BlockSpec(memory_space=pl.ANY)
    B = BLOCKS

    def buf(*shape, dtype=F32):
        return pltpu.VMEM(shape, dtype)

    stream, finals = pl.pallas_call(
        functools.partial(whole_kernel, ntp, ndp, steps, features, cap, share, live_rows, lag, halves),
        out_shape=(
            pltpu.VMEM((cap, depth), F32),
            pltpu.VMEM(states.shape, F32),
        ),
        in_specs=[hbm] * 13,
        out_specs=(vmem, vmem),
        scratch_shapes=[
            pltpu.SMEM(lengths.shape, jnp.int32),
            buf(B, depth), buf(B, span), buf(B, span),
            buf(B, 6, depth, span, dtype=BF16),
            buf(B, span, depth, dtype=BF16),
            buf(*states.shape),
            buf(ntp, cap, depth, dtype=BF16),
            buf(ntp, share, depth, dtype=BF16),
            buf(cap, depth, dtype=BF16),
            buf(ntp, 8, packed),
            buf(ndp, 8, every), buf(ndp, 8, packed),
            buf(every, LANES), buf(packed, LANES),
            buf(halves, packed, every // halves, dtype=BF16), buf(every, packed, dtype=BF16),
            buf(ntp, pieces, cap, wide), buf(ntp, pieces, share, wide),
            buf(ntp, pieces, cap // CORES, wide), buf(ntp, pieces, share // CORES, wide),
            buf(ntp, pieces, cap // CORES, wide, dtype=BF16),
            buf(ntp, pieces, share // CORES, wide, dtype=BF16),
            buf(nx, ntp, pieces, cap // CORES, wide, dtype=BF16),
            buf(nx, ntp, pieces, share // CORES, wide, dtype=BF16),
            buf(pieces, rows, wide), buf(pieces, packed, wide),
            buf(B, halves, ndp, rows // halves, span, dtype=BF16),
            buf(halves, ntp, cap // halves, depth, dtype=BF16),
            buf(halves, ntp, cap // halves, depth, dtype=BF16),
            buf(1, ntp, share, depth, dtype=BF16),
            buf(1, ntp, share, depth, dtype=BF16),
            buf(halves, held * tall // halves, LANES),
            buf(halves, held * tall // halves, LANES),
            buf(halves, held * tall // halves, LANES),
            buf(halves, held // halves, 2 * tall, span, dtype=BF16),
            buf(halves, held // halves, 2 * tall, LANES),
            dma((7,)), dma((B, 6)),
            dma((2, ntp)), dma((2, ntp)), dma((ntp,)), dma((ntp,)),
            dma((B, count)), dma((B, count)),
            dma((B, nx, count)), dma((B, nx, count)),
            dma((B, count)), dma((B, count)),
            dma((B, ndp)), dma((B, ndp)),
            dma((B, halves, ndp)), dma((B, halves, ndp)), dma((B, halves, ntp)), dma((B, halves, ntp)),
        ],
        compiler_params=pltpu.CompilerParams(
            collective_id=0, has_side_effects=True, vmem_limit_bytes=56 * 1024 * 1024
        ),
        name="whole",
    )(
        *(
            pltpu.with_memory_space_constraint(a, pltpu.HBM)
            for a in (
                tokens.reshape(cap, depth), lengths, norm_gain,
                w_recept, w_key, w_value, w_decay, w_rate, w_gate,
                w_out, decay_base, out_gain, states,
            )
        )
    )
    return stream.reshape(tokens.shape), finals


def solution(mesh):
    in_specs = (
        P(("grp", "tp"), None, "dp"),
        P("grp"),
        P(None, "dp"),
        P(None, "dp", "tp"),
        P(None, "dp", "tp"),
        P(None, "dp", "tp"),
        P(None, "dp", "tp"),
        P(None, "dp", "tp"),
        P(None, "dp", "tp"),
        P(None, "tp", "dp"),
        P(None, "tp"),
        P(None, "tp"),
        P(None, ("grp", "dp"), None, "tp"),
    )
    out_specs = (P(("grp", "tp"), None, "dp"), P(None, ("grp", "dp"), None, "tp"))
    run = functools.partial(body, mesh.shape["tp"], mesh.shape["dp"])
    return jax.shard_map(run, mesh=mesh, in_specs=in_specs, out_specs=out_specs, check_vma=False)
```
